32 devices in a mesh: fs: 16 (over z, y, x), tp: 2 (over core).
Axes of the slice: x: 2, y: 2, z: 4, core: 2. Of those that a mesh axis runs over, the one named last changes fastest.
Arguments:
- tokens: bfloat16 [4096, 1024], P('fs', 'tp'), may hold values from -6 to 6
- mix_gain: float32 [1024], replicated, may hold values from 0.1 to 1.9
- mix_value_w: float32 [1024, 1024], P('fs', 'tp'), may hold values from -0.1875 to 0.1875
- mix_gate_w: float32 [1024, 1024], P('fs', 'tp'), may hold values from -0.1875 to 0.1875
- mix_kernel: float32 [31, 1024], P(None, 'tp'), may hold values from -1 to 1
- chan_gain: float32 [1024], P('tp'), may hold values from 0.1 to 1.9
- chan_bias: float32 [1024], P('tp'), may hold values from -3 to 3
- mix_out_w: float32 [1024, 1024], P('tp', 'fs'), may hold values from -0.1875 to 0.1875
- ffn_gain: float32 [1024], replicated, may hold values from 0.1 to 1.9
- ffn_value_w: float32 [1024, 2560], P('fs', 'tp'), may hold values from -0.1875 to 0.1875
- ffn_gate_w: float32 [1024, 2560], P('fs', 'tp'), may hold values from -0.1875 to 0.1875
- ffn_value_kernel: float32 [3, 2560], P(None, 'tp'), may hold values from -3.5 to 3.5
- ffn_gate_kernel: float32 [3, 2560], P(None, 'tp'), may hold values from -3.5 to 3.5
- ffn_down_w: float32 [2560, 1024], P('tp', 'fs'), may hold values from -0.125 to 0.125
Outputs:
- layer_out: bfloat16 [4096, 1024], P('fs', 'tp')
The draws below stay inside these ranges and needn't reach their ends.
All inputs are finite; a program needn't handle non-finite values.
Results may differ from the reference program's by a relative error of at most 0.0035.
Values may be sent and summed in bfloat16 or wider, within the bound.
A program may use at most 64 MiB of HBM per device.

```python
import jax
import jax.numpy as jnp
from jax import lax

D = 1024
CONV_W = 1024
FFN_W = 2560
CONV_K = 31
FFN_K = 3
SEQ_LEN = 32
TOKENS = 4096


def level_of(stream_key, extent, split, low, top_value):
    loudness, own = 1.0, jax.random.fold_in(stream_key, 6)
    for axis_at, parts in split:
        heights = jnp.exp(jax.random.uniform(jax.random.fold_in(own, axis_at), (parts,), jnp.float32, low / len(split), top_value / len(split)))
        loudness = loudness * jnp.repeat(heights, extent[axis_at] // parts).reshape([-1 if axis == axis_at else 1 for axis in range(len(extent))])
    return loudness


def gaussian(key, dims, spread, limit, pieces=(), kind=jnp.bfloat16):
    level = level_of(key, dims, pieces, -0.22, 0.18) if pieces else 1.0
    drawn = jax.random.normal(key, dims, jnp.float32) * spread * level
    return jnp.minimum(jnp.maximum(drawn, -limit), limit).astype(kind)


def setup_inputs(seed: int = 0) -> dict:
    keys = jax.random.split(jax.random.key(seed), 15)
    return {
        "tokens": gaussian(keys[0], (TOKENS, D), 1.0, 6.0, ((0, 16), (1, 2))),
        "mix_gain": jnp.clip(1.0 + 0.18 * jax.random.normal(keys[1], (D,), jnp.float32), 0.1, 1.9),
        "mix_value_w": gaussian(keys[2], (D, CONV_W), D ** -0.5, 0.1875, ((0, 16), (1, 2)), jnp.float32),
        "mix_gate_w": gaussian(keys[3], (D, CONV_W), D ** -0.5, 0.1875, ((0, 16), (1, 2)), jnp.float32),
        "mix_kernel": gaussian(keys[4], (CONV_K, CONV_W), CONV_K ** -0.5, 1.0, ((1, 2),), jnp.float32),
        "chan_gain": jnp.clip(1.0 + 0.18 * jax.random.normal(keys[5], (CONV_W,), jnp.float32), 0.1, 1.9),
        "chan_bias": gaussian(keys[6], (CONV_W,), 0.5, 3.0, ((0, 2),), jnp.float32),
        "mix_out_w": gaussian(keys[7], (CONV_W, D), CONV_W ** -0.5, 0.1875, ((0, 2), (1, 16)), jnp.float32),
        "ffn_gain": jnp.clip(1.0 + 0.18 * jax.random.normal(keys[8], (D,), jnp.float32), 0.1, 1.9),
        "ffn_value_w": gaussian(keys[9], (D, FFN_W), D ** -0.5, 0.1875, ((0, 16), (1, 2)), jnp.float32),
        "ffn_gate_w": gaussian(keys[10], (D, FFN_W), D ** -0.5, 0.1875, ((0, 16), (1, 2)), jnp.float32),
        "ffn_value_kernel": gaussian(keys[11], (FFN_K, FFN_W), FFN_K ** -0.5, 3.5, ((1, 2),), jnp.float32),
        "ffn_gate_kernel": gaussian(keys[12], (FFN_K, FFN_W), FFN_K ** -0.5, 3.5, ((1, 2),), jnp.float32),
        "ffn_down_w": gaussian(keys[13], (FFN_W, D), FFN_W ** -0.5, 0.125, ((0, 2), (1, 16)), jnp.float32),
    }


EPS = 1e-06

def rms_rows(act_rows, norm_gain):
    values = act_rows.astype(jnp.float32)
    scaled = values * lax.rsqrt(lax.optimization_barrier(jnp.mean(values * values, axis=-1, keepdims=True)) + EPS)
    return (scaled * norm_gain).astype(jnp.bfloat16)

def along_positions(values, kernel, length):
    seq_count = values.shape[0] // length
    blocks = values.reshape(seq_count, length, values.shape[1])
    half_width = kernel.shape[0] // 2
    padded = jnp.pad(blocks, ((0, 0), (half_width, half_width), (0, 0)))
    summed = jnp.zeros_like(blocks)
    for offset in range(kernel.shape[0]):
        summed = summed + padded[:, offset:offset + length, :] * kernel[offset]
    return summed.reshape(values.shape)

def matmul_bf(left, weight):
    return jnp.dot(left, weight.astype(jnp.bfloat16), preferred_element_type=jnp.float32)

def reference(tokens, mix_gain, mix_value_w, mix_gate_w, mix_kernel, chan_gain, chan_bias, mix_out_w, ffn_gain, ffn_value_w, ffn_gate_w, ffn_value_kernel, ffn_gate_kernel, ffn_down_w):
    normed = rms_rows(tokens, mix_gain)
    glu_rows = matmul_bf(normed, mix_value_w) * jax.nn.sigmoid(matmul_bf(normed, mix_gate_w))
    mixed = along_positions(glu_rows, mix_kernel, SEQ_LEN)
    chan_mean = lax.optimization_barrier(jnp.mean(mixed, axis=-1, keepdims=True))
    chan_var = lax.optimization_barrier(jnp.mean(jnp.square(mixed - chan_mean), axis=-1, keepdims=True))
    active = jax.nn.silu((mixed - chan_mean) * lax.rsqrt(chan_var + EPS) * chan_gain + chan_bias).astype(jnp.bfloat16)
    middle = (tokens.astype(jnp.float32) + matmul_bf(active, mix_out_w)).astype(jnp.bfloat16)
    normed_ffn = rms_rows(middle, ffn_gain)
    up_value = along_positions(matmul_bf(normed_ffn, ffn_value_w), ffn_value_kernel, SEQ_LEN)
    up_gate = along_positions(matmul_bf(normed_ffn, ffn_gate_w), ffn_gate_kernel, SEQ_LEN)
    hidden = (jax.nn.silu(up_gate) * up_value).astype(jnp.bfloat16)
    return (middle.astype(jnp.float32) + matmul_bf(hidden, ffn_down_w)).astype(jnp.bfloat16)
```

```python
import jax
import jax.numpy as jnp
from jax import lax
from jax.sharding import PartitionSpec as P

CONV_W = 1024
SEQ_LEN = 32


EPS = 1e-06


def rms_rows(act_rows, norm_gain):
    values = act_rows.astype(jnp.float32)
    scaled = values * lax.rsqrt(jnp.mean(values * values, axis=-1, keepdims=True) + EPS)
    return (scaled * norm_gain).astype(jnp.bfloat16)


def along_positions(values, kernel, length):
    seq_count = values.shape[0] // length
    blocks = values.reshape(seq_count, length, values.shape[1])
    half_width = kernel.shape[0] // 2
    padded = jnp.pad(blocks, ((0, 0), (half_width, half_width), (0, 0)))
    summed = jnp.zeros_like(blocks)
    for offset in range(kernel.shape[0]):
        summed = summed + padded[:, offset : offset + length, :] * kernel[offset]
    return summed.reshape(values.shape)


def collect_rows(local_rows):
    return lax.all_gather(local_rows, "tp", axis=1, tiled=True)


def project_in(normed, weight_one, weight_two):
    empty = jnp.zeros((normed.shape[0], weight_one.shape[1]), jnp.float32)

    def add_both(totals, pieces):
        columns = lax.slice_in_dim(normed, 0, pieces[0].shape[0], axis=1)
        first = totals[0] + jnp.dot(
            columns, pieces[0].astype(jnp.bfloat16), preferred_element_type=jnp.float32
        )
        second = totals[1] + jnp.dot(
            columns, pieces[1].astype(jnp.bfloat16), preferred_element_type=jnp.float32
        )
        return (first, second)

    return add_both(
        (empty, empty),
        (
            lax.all_gather(weight_one.astype(jnp.bfloat16), "fs", axis=0, tiled=True),
            lax.all_gather(weight_two.astype(jnp.bfloat16), "fs", axis=0, tiled=True),
        ),
    )


def project_out(active, weight):

    def apply_piece(piece):
        return jnp.dot(active, piece.astype(jnp.bfloat16), preferred_element_type=jnp.float32)

    partial_terms = apply_piece(lax.all_gather(weight.astype(jnp.bfloat16), "fs", axis=1, tiled=True))
    return lax.psum_scatter(partial_terms, "tp", scatter_dimension=1, tiled=True)


def body(
    tokens,
    mix_gain,
    mix_value_w,
    mix_gate_w,
    mix_kernel,
    chan_gain,
    chan_bias,
    mix_out_w,
    ffn_gain,
    ffn_value_w,
    ffn_gate_w,
    ffn_value_kernel,
    ffn_gate_kernel,
    ffn_down_w,
):
    normed = rms_rows(collect_rows(tokens), mix_gain)
    mix_value, mix_gate = project_in(normed, mix_value_w, mix_gate_w)
    glu_rows = mix_value * jax.nn.sigmoid(mix_gate)
    mixed = along_positions(glu_rows, mix_kernel, SEQ_LEN)
    chan_sum, chan_square = lax.psum(
        (jnp.sum(mixed, axis=-1), jnp.sum(mixed * mixed, axis=-1)), "tp"
    )
    chan_mean = (chan_sum / CONV_W)[:, None]
    chan_var = jnp.maximum((chan_square / CONV_W)[:, None] - chan_mean * chan_mean, 0.0)
    active = jax.nn.silu(
        (mixed - chan_mean) * lax.rsqrt(chan_var + EPS) * chan_gain + chan_bias
    ).astype(jnp.bfloat16)
    middle = (tokens.astype(jnp.float32) + project_out(active, mix_out_w)).astype(jnp.bfloat16)
    normed_ffn = rms_rows(collect_rows(middle), ffn_gain)
    up_value, up_gate = project_in(normed_ffn, ffn_value_w, ffn_gate_w)
    up_value = along_positions(up_value, ffn_value_kernel, SEQ_LEN)
    up_gate = along_positions(up_gate, ffn_gate_kernel, SEQ_LEN)
    hidden = (jax.nn.silu(up_gate) * up_value).astype(jnp.bfloat16)
    return (middle.astype(jnp.float32) + project_out(hidden, ffn_down_w)).astype(jnp.bfloat16)


def solution(mesh):
    return jax.shard_map(
        body,
        mesh=mesh,
        in_specs=(
            P("fs", "tp"),
            P(),
            P("fs", "tp"),
            P("fs", "tp"),
            P(None, "tp"),
            P("tp"),
            P("tp"),
            P("tp", "fs"),
            P(),
            P("fs", "tp"),
            P("fs", "tp"),
            P(None, "tp"),
            P(None, "tp"),
            P("tp", "fs"),
        ),
        out_specs=P("fs", "tp"),
        check_vma=False,
    )
```

```python
import functools

import jax
import jax.numpy as jnp
from jax import lax
from jax.experimental import pallas as pl
from jax.experimental.pallas import tpu as pltpu
from jax.sharding import PartitionSpec as P

CONV_W = 1024
SEQ_LEN = 32


EPS = 1e-06


def rms_rows(act_rows, norm_gain):
    values = act_rows.astype(jnp.float32)
    scaled = values * lax.rsqrt(jnp.mean(values * values, axis=-1, keepdims=True) + EPS)
    return (scaled * norm_gain).astype(jnp.bfloat16)


def along_positions(values, kernel, length):
    seq_count = values.shape[0] // length
    blocks = values.reshape(seq_count, length, values.shape[1])
    half_width = kernel.shape[0] // 2
    padded = jnp.pad(blocks, ((0, 0), (half_width, half_width), (0, 0)))
    summed = jnp.zeros_like(blocks)
    for offset in range(kernel.shape[0]):
        summed = summed + padded[:, offset : offset + length, :] * kernel[offset]
    return summed.reshape(values.shape)


def collect_rows(local_rows):
    return lax.all_gather(local_rows, "tp", axis=1, tiled=True)


def project_in(normed, weight_one, weight_two):
    empty = jnp.zeros((normed.shape[0], weight_one.shape[1]), jnp.float32)

    def add_both(totals, pieces):
        columns = lax.slice_in_dim(normed, 0, pieces[0].shape[0], axis=1)
        first = totals[0] + jnp.dot(
            columns, pieces[0].astype(jnp.bfloat16), preferred_element_type=jnp.float32
        )
        second = totals[1] + jnp.dot(
            columns, pieces[1].astype(jnp.bfloat16), preferred_element_type=jnp.float32
        )
        return (first, second)

    return add_both(
        (empty, empty),
        (
            lax.all_gather(weight_one.astype(jnp.bfloat16), "fs", axis=0, tiled=True),
            lax.all_gather(weight_two.astype(jnp.bfloat16), "fs", axis=0, tiled=True),
        ),
    )


def project_out(active, weight):

    def apply_piece(piece):
        return jnp.dot(active, piece.astype(jnp.bfloat16), preferred_element_type=jnp.float32)

    partial_terms = apply_piece(lax.all_gather(weight.astype(jnp.bfloat16), "fs", axis=1, tiled=True))
    return lax.psum_scatter(partial_terms, "tp", scatter_dimension=1, tiled=True)


def body(
    tokens,
    mix_gain,
    mix_value_w,
    mix_gate_w,
    mix_kernel,
    chan_gain,
    chan_bias,
    mix_out_w,
    ffn_gain,
    ffn_value_w,
    ffn_gate_w,
    ffn_value_kernel,
    ffn_gate_kernel,
    ffn_down_w,
):
    normed = rms_rows(collect_rows(tokens), mix_gain)
    mix_value, mix_gate = project_in(normed, mix_value_w, mix_gate_w)
    glu_rows = mix_value * jax.nn.sigmoid(mix_gate)
    mixed = along_positions(glu_rows, mix_kernel, SEQ_LEN)
    chan_sum, chan_square = lax.psum(
        (jnp.sum(mixed, axis=-1), jnp.sum(mixed * mixed, axis=-1)), "tp"
    )
    chan_mean = (chan_sum / CONV_W)[:, None]
    chan_var = jnp.maximum((chan_square / CONV_W)[:, None] - chan_mean * chan_mean, 0.0)
    active = jax.nn.silu(
        (mixed - chan_mean) * lax.rsqrt(chan_var + EPS) * chan_gain + chan_bias
    ).astype(jnp.bfloat16)
    middle = (tokens.astype(jnp.float32) + project_out(active, mix_out_w)).astype(jnp.bfloat16)
    normed_ffn = rms_rows(collect_rows(middle), ffn_gain)
    up_value, up_gate = project_in(normed_ffn, ffn_value_w, ffn_gate_w)
    up_value = along_positions(up_value, ffn_value_kernel, SEQ_LEN)
    up_gate = along_positions(up_gate, ffn_gate_kernel, SEQ_LEN)
    hidden = (jax.nn.silu(up_gate) * up_value).astype(jnp.bfloat16)
    return (middle.astype(jnp.float32) + project_out(hidden, ffn_down_w)).astype(jnp.bfloat16)


MESH = pl.DeviceIdType.MESH
UNIT_US = 0.36
HOP_US = 1.8


def chunk_plan(mix_cols, ffn_cols):
    unit = 256
    first = max(unit, (2 * ffn_cols // 5) // unit * unit)
    rest = ffn_cols - 2 * first
    plan = [
        ("mv", "A", mix_cols, True),
        ("mg", "B", mix_cols, True),
        ("v0", "A", first, False),
        ("g0", "B", first, False),
        ("mo", "D", mix_cols, False),
        ("v1", "A", first, False),
        ("g1", "B", first, False),
        ("w0", "A", first, False),
        ("w1", "B", first, False),
        ("vg2", "E", 2 * rest, False),
        ("w2", "D", rest, False),
    ]
    gates = {
        "v1": ("mo", "u", 2),
        "g1": ("mo", "u", 2),
        "w0": ("v1", "u", 1),
        "w1": ("g1", "u", 1),
        "vg2": ("w0", "u", 2),
        "w2": ("vg2", "u", 1),
    }
    return plan, gates


def build_transfers(plan, gates, line):
    out = {}
    for name, kind, cols, fine in plan:
        width = cols // 128
        gate = [gates[name]] if name in gates else []
        steps = range(1, line)
        if kind in "AB":
            one, two = ("y", "x") if kind == "A" else ("x", "y")
            for t in steps:
                for d in "ud":
                    deps = [(name, d, t - 1)] if t > 1 else gate
                    out[(name, d, t)] = dict(link="z" + d, size=width, deps=deps, phase="z")
            everything = [(name, d, t) for t in steps for d in "ud"]
            if fine:
                out[(name, "1", "o", 0)] = dict(link=one, size=width, deps=[], phase="f1", axis=one)
                out[(name, "2", "o", 0)] = dict(
                    link=two, size=2 * width, deps=[(name, "1", "o", 0)], phase="f2", axis=two
                )
                for _, d, t in everything:
                    out[(name, "1", d, t)] = dict(link=one, size=width, deps=[(name, d, t)], phase="f1", axis=one)
                    out[(name, "2", d, t)] = dict(
                        link=two, size=2 * width, deps=[(name, "1", d, t)], phase="f2", axis=two
                    )
            else:
                out[(name, "1")] = dict(link=one, size=line * width, deps=everything, phase="c1", axis=one)
                out[(name, "2")] = dict(link=two, size=2 * line * width, deps=[(name, "1")], phase="c2", axis=two)
        else:
            one, two = ("x", "y") if kind == "D" else ("y", "x")
            out[(name, "1")] = dict(link=one, size=width, deps=[], phase="p1", axis=one)
            out[(name, "2")] = dict(link=two, size=2 * width, deps=[(name, "1")], phase="p2", axis=two)
            for t in steps:
                for d in "ud":
                    deps = [(name, d, t - 1)] if t > 1 else [(name, "2")] + gate
                    out[(name, d, t)] = dict(link="z" + d, size=4 * width, deps=deps, phase="q")
    return out


def order_events(transfers, computes):
    free, arrival, seen, done = {}, {}, set(), set()
    program, now = [], 0.0

    def issue():
        for key, item in transfers.items():
            if key not in arrival and all(dep in seen for dep in item["deps"]):
                start = max(now, free.get(item["link"], 0.0))
                free[item["link"]] = start + item["size"] * UNIT_US
                arrival[key] = free[item["link"]] + HOP_US
                program.append(("send", key))

    issue()
    program.append(("local", None))
    while len(seen) < len(transfers) or len(done) < len(computes):
        waiting = sorted((arrival[key], i, key) for i, key in enumerate(transfers) if key in arrival and key not in seen)
        ready = None
        for name, needs, after, cost in computes:
            if name in done:
                continue
            chunk_ok = all(key in seen for key in transfers if key[0] in needs)
            if chunk_ok and all(a in done for a in after):
                ready = (name, cost)
                break
        if waiting and waiting[0][0] <= now or (waiting and ready is None):
            now = max(now, waiting[0][0])
            seen.add(waiting[0][2])
            program.append(("recv", waiting[0][2]))
            issue()
        else:
            program.append(("compute", ready[0]))
            now += ready[1]
            done.add(ready[0])
    return program


def compute_list(groups):
    items = [
        ("norm1", (), (), 1.0),
        ("mixv", ("mv",), ("norm1",), 0.8),
        ("mixg", ("mg",), ("mixv",), 1.0),
        ("conv_a", (), ("mixg",), 1.5),
        ("conv_b", (), ("conv_a",), 1.5),
        ("stats", (), ("conv_b",), 0.5),
        ("active", (), ("stats",), 1.5),
        ("out_peer", ("mo",), ("active",), 0.6),
        ("out_mine", (), ("out_peer",), 0.6),
        ("middle", (), ("out_mine",), 1.0),
        ("norm2", (), ("middle",), 1.5),
        ("up0", ("v0", "g0"), ("norm2",), 2.0),
        ("up1", ("v1", "g1"), ("norm2",), 2.0),
        ("up2", ("vg2",), ("norm2",), 1.0),
    ]
    for g in (0, 1, 2):
        items.append(("down_peer%d" % g, ("w%d" % g,), ("up%d" % g,), 0.5))
    items.append(("send_down", (), tuple("down_peer%d" % g for g in (0, 1, 2)), 0.1))
    for g in (0, 1, 2):
        items.append(("down_mine%d" % g, (), ("send_down",), 0.5))
    items.append(("finish", (), tuple("down_mine%d" % g for g in (0, 1, 2)), 1.0))
    return items


def layer_kernel(sizes, plan, transfers, program, *refs):
    line, rows, tok_rows, mix_cols, ffn_cols, width, taps, ffn_taps = sizes
    (tokens, gain1, kern, cgain, cbias, gain2, vkern, gkern, packed) = refs[:9]
    out = refs[9]
    scratch = refs[10:]
    held = {item[0]: scratch[i] for i, item in enumerate(plan)}
    (tok_peer, normed, mvbuf, pad, mixed, stat, stat_peer, active, part_send, part_mine, part_recv,
     middle, mid_peer, hid0, hid1, hid2, down_send, down_mine, down_recv,
     send_sem, recv_sem, loc_sem, tp_send, tp_recv) = scratch[len(plan):]
    hidden = (hid0, hid1, hid2)
    offsets, at = {}, 0
    for name, _, cols, _ in plan:
        offsets[name] = at
        at += cols
    cols_of = {item[0]: item[2] for item in plan}
    numbers = {key: i for i, key in enumerate(transfers)}
    fs = lax.axis_index("fs")
    core = lax.axis_index("tp")
    peer = 1 - core
    z, y, x = lax.div(fs, 4), lax.rem(lax.div(fs, 2), 2), lax.rem(fs, 2)
    at_y, at_x = fs + 2 - 4 * y, fs + 1 - 2 * x
    half = line // 2

    barrier = pltpu.get_barrier_semaphore()
    for dev in ({"fs": at_y}, {"fs": at_x}, {"tp": peer}):
        pl.semaphore_signal(barrier, inc=1, device_id=dev, device_id_type=MESH)

    @pl.when(z > 0)
    def _():
        pl.semaphore_signal(barrier, inc=1, device_id={"fs": fs - 4}, device_id_type=MESH)

    @pl.when(z < line - 1)
    def _():
        pl.semaphore_signal(barrier, inc=1, device_id={"fs": fs + 4}, device_id_type=MESH)

    local = []
    for i, (name, _, cols, _) in enumerate(plan):
        copy = pltpu.make_async_copy(
            packed.at[:, pl.ds(offsets[name], cols)], held[name].at[z, y, x], loc_sem.at[i]
        )
        copy.start()
        local.append(copy)
    pl.semaphore_wait(barrier, 3 + jnp.minimum(z, 1) + jnp.minimum(line - 1 - z, 1))

    def guards(key, sending):
        phase = transfers[key]["phase"]
        if phase in ("z", "q"):
            d, t = key[1], key[2]
            if d == "u":
                return jnp.logical_and(z >= t - 1, z < line - 1) if sending else z >= t
            return jnp.logical_and(z <= line - t, z > 0) if sending else z <= line - 1 - t
        if phase in ("f1", "f2") and key[2] != "o":
            d, t = key[2], key[3]
            return z >= t if d == "u" else z <= line - 1 - t
        return None

    def make(key, sending):
        item = transfers[key]
        phase, name, i = item["phase"], key[0], numbers[key]
        buf = held[name]
        own = packed.at[:, pl.ds(offsets[name], cols_of[name])]
        src = None
        if phase in ("z", "q"):
            d, t = key[1], key[2]
            back = t - 1 if sending else t
            block = z - back if d == "u" else z + back
            dev = {"fs": fs + 4 if d == "u" else fs - 4}
            if phase == "z":
                dst = buf.at[block, y, x]
                src = own if sending and t == 1 else dst
            else:
                dst = buf.at[block]
        else:
            axis = item["axis"]
            dev = {"fs": at_y if axis == "y" else at_x}
            yy, xx = y, x
            if not sending:
                yy, xx = (1 - y, x) if axis == "y" else (y, 1 - x)
            if phase in ("f1", "f2"):
                d, t = key[2], key[3]
                block = z - t if d == "u" else z + t
            elif phase in ("p1", "p2"):
                block = z
            else:
                block = slice(None)
            if phase in ("f1", "p1", "c1"):
                dst = buf.at[block, yy, xx]
                if sending and (phase == "p1" or (phase == "f1" and key[2] == "o")):
                    src = own
            elif axis == "x":
                dst = buf.at[block, :, xx]
            else:
                dst = buf.at[block, yy, :]
        return pltpu.make_async_remote_copy(
            src_ref=dst if src is None else src, dst_ref=dst, send_sem=send_sem.at[i],
            recv_sem=recv_sem.at[i], device_id=dev, device_id_type=MESH,
        )

    def act(key, sending, what):
        guard = guards(key, sending)

        def run():
            what(make(key, sending))

        if guard is None:
            run()
        else:
            pl.when(guard)(run)

    def to_peer(i, src, dst):
        return pltpu.make_async_remote_copy(
            src_ref=src, dst_ref=dst, send_sem=tp_send.at[i], recv_sem=tp_recv.at[i],
            device_id={"tp": peer}, device_id_type=MESH,
        )

    tok_copy = to_peer(0, tokens, tok_peer)
    tok_copy.start()
    stat_copy = to_peer(1, stat, stat_peer)
    part_copy = to_peer(2, part_send, part_recv)
    mid_copy = to_peer(3, middle, mid_peer)
    down_copy = to_peer(4, down_send, down_recv)

    def norm_rows(mine, other, gain):
        def block(r, carry):
            at_rows = pl.ds(pl.multiple_of(r * 32, 32), 32)
            a = mine[at_rows, :].astype(jnp.float32)
            b = other[at_rows, :].astype(jnp.float32)
            total = jnp.sum(a * a, axis=-1, keepdims=True) + jnp.sum(b * b, axis=-1, keepdims=True)
            scale = lax.rsqrt(total / width + EPS)
            normed[core, at_rows, :] = (a * scale * gain[core]).astype(jnp.bfloat16)
            normed[peer, at_rows, :] = (b * scale * gain[peer]).astype(jnp.bfloat16)
            return carry

        lax.fori_loop(0, tok_rows // 32, block, 0)

    def project(name, cols):
        total = None
        for h in (0, 1):
            weight = held[name][h * half:(h + 1) * half, :, :, :, cols]
            weight = weight.reshape(-1, weight.shape[-1])
            term = jnp.dot(normed[h], weight, preferred_element_type=jnp.float32)
            total = term if total is None else total + term
        return total

    def project_back(left, name, side):
        weight = held[name][pl.ds(side * half, half)]
        weight = weight.reshape(-1, weight.shape[-1])
        return lax.dot_general(left, weight, (((1,), (1,)), ((), ())), preferred_element_type=jnp.float32)

    def norm1():
        tok_copy.wait_recv()
        pad[...] = jnp.zeros_like(pad)
        norm_rows(tokens, tok_peer, gain1)

    def mixv():
        for c in range(0, mix_cols, 256):
            mvbuf[:, c:c + 256] = project("mv", slice(c, c + 256))

    seqs = tok_rows // SEQ_LEN
    lead = -(-(taps // 2) // 8) * 8

    def mixg():
        for c in range(0, mix_cols, 256):
            glu = mvbuf[:, c:c + 256] * jax.nn.sigmoid(project("mg", slice(c, c + 256)))
            pad[:, lead:lead + SEQ_LEN, c:c + 256] = glu.reshape(seqs, SEQ_LEN, 256)

    def conv(lo, hi):
        def block(i, carry):
            s, c = lax.div(i, hi - lo), lo + lax.rem(i, hi - lo)
            lanes = pl.ds(pl.multiple_of(c * 128, 128), 128)
            total = jnp.zeros((SEQ_LEN, 128), jnp.float32)
            for k in range(taps):
                total = total + pad[s, pl.ds(lead - taps // 2 + k, SEQ_LEN), lanes] * kern[k:k + 1, lanes]
            mixed[pl.ds(pl.multiple_of(s * SEQ_LEN, SEQ_LEN), SEQ_LEN), lanes] = total
            return carry

        lax.fori_loop(0, seqs * (hi - lo), block, 0)

    lane_blocks = mix_cols // 128

    def stats():
        def block(r, carry):
            at_rows = pl.ds(pl.multiple_of(r * 64, 64), 64)
            v = mixed[at_rows, :]
            first = jnp.sum(v, axis=-1, keepdims=True)
            second = jnp.sum(v * v, axis=-1, keepdims=True)
            lane = lax.broadcasted_iota(jnp.int32, (64, 128), 1)
            stat[at_rows, :] = jnp.where(lane == 0, first, second)
            return carry

        lax.fori_loop(0, tok_rows // 64, block, 0)
        stat_copy.start()

    def make_active():
        stat_copy.wait_recv()

        def block(r, carry):
            at_rows = pl.ds(pl.multiple_of(r * 32, 32), 32)
            both = stat[at_rows, :] + stat_peer[at_rows, :]
            mean = both[:, 0:1] / (2 * mix_cols)
            var = jnp.maximum(both[:, 1:2] / (2 * mix_cols) - mean * mean, 0.0)
            v = (mixed[at_rows, :] - mean) * lax.rsqrt(var + EPS) * cgain[...] + cbias[...]
            active[at_rows, :] = (v * jax.nn.sigmoid(v)).astype(jnp.bfloat16)
            return carry

        lax.fori_loop(0, tok_rows // 32, block, 0)

    def out_peer():
        part_send[...] = project_back(active[...], "mo", peer)
        part_copy.start()

    def out_mine():
        part_mine[...] = project_back(active[...], "mo", core)

    def make_middle():
        part_copy.wait_recv()
        middle[...] = (tokens[...].astype(jnp.float32) + (part_mine[...] + part_recv[...])).astype(jnp.bfloat16)
        mid_copy.start()

    def norm2():
        mid_copy.wait_recv()
        norm_rows(middle, mid_peer, gain2)

    def short_conv(values, kernel_rows):
        pos = lax.rem(lax.broadcasted_iota(jnp.int32, values.shape, 0), SEQ_LEN)
        total = None
        for k in range(ffn_taps):
            shift = k - ffn_taps // 2
            term = values
            if shift:
                term = pltpu.roll(values, (-shift) % tok_rows, 0)
                inside = pos < SEQ_LEN - shift if shift > 0 else pos >= -shift
                term = jnp.where(inside, term, 0.0)
            term = term * kernel_rows[k:k + 1, :]
            total = term if total is None else total + term
        return total

    first = cols_of["v0"]

    def up(g):
        count = hidden[g].shape[1]
        for c in range(0, count, 256):
            at_cols = slice(g * first + c, g * first + c + 256)
            if g < 2:
                value = project("v%d" % g, slice(c, c + 256))
                gate = project("g%d" % g, slice(c, c + 256))
            else:
                value = project("vg2", slice(c, c + 256))
                gate = project("vg2", slice(count + c, count + c + 256))
            value = short_conv(value, vkern[:, at_cols])
            gate = short_conv(gate, gkern[:, at_cols])
            hidden[g][:, c:c + 256] = (gate * jax.nn.sigmoid(gate) * value).astype(jnp.bfloat16)

    fresh = {"peer": True, "mine": True}

    def down(g, side, which, buf):
        term = project_back(hidden[g][...], "w%d" % g, side)
        if fresh[which]:
            buf[...] = term
        else:
            buf[...] += term
        fresh[which] = False

    def finish():
        down_copy.wait_recv()
        total = middle[...].astype(jnp.float32) + (down_mine[...] + down_recv[...])
        out[...] = total.astype(jnp.bfloat16)

    run = {
        "norm1": norm1, "mixv": mixv, "mixg": mixg,
        "conv_a": lambda: conv(0, lane_blocks // 2),
        "conv_b": lambda: conv(lane_blocks // 2, lane_blocks),
        "stats": stats, "active": make_active, "out_peer": out_peer, "out_mine": out_mine,
        "middle": make_middle, "norm2": norm2, "send_down": lambda: down_copy.start(), "finish": finish,
    }
    for g in (0, 1, 2):
        run["up%d" % g] = functools.partial(up, g)
        run["down_peer%d" % g] = functools.partial(down, g, peer, "peer", down_send)
        run["down_mine%d" % g] = functools.partial(down, g, core, "mine", down_mine)

    for kind, key in program:
        if kind == "send":
            act(key, True, lambda copy: copy.start())
        elif kind == "recv":
            act(key, False, lambda copy: copy.wait_recv())
        elif kind == "local":
            for copy in local:
                copy.wait()
        else:
            run[key]()
    for key in transfers:
        act(key, True, lambda copy: copy.wait_send())
    for copy in (tok_copy, stat_copy, part_copy, mid_copy, down_copy):
        copy.wait_send()


def fused_body(fs_size, tokens, mix_gain, mix_value_w, mix_gate_w, mix_kernel, chan_gain, chan_bias, mix_out_w,
               ffn_gain, ffn_value_w, ffn_gate_w, ffn_value_kernel, ffn_gate_kernel, ffn_down_w):
    rows, mix_cols = mix_value_w.shape
    ffn_cols = ffn_value_w.shape[1]
    tok_rows, tok_cols = tokens.shape
    line = fs_size // 4
    plan, gates = chunk_plan(mix_cols, ffn_cols)
    transfers = build_transfers(plan, gates, line)
    program = order_events(transfers, compute_list(3))
    first = [item[2] for item in plan if item[0] == "v0"][0]
    rest = ffn_cols - 2 * first
    v, g, w = ffn_value_w, ffn_gate_w, ffn_down_w.T
    pieces = {
        "mv": [mix_value_w], "mg": [mix_gate_w], "mo": [mix_out_w.T],
        "v0": [v[:, :first]], "v1": [v[:, first:2 * first]],
        "g0": [g[:, :first]], "g1": [g[:, first:2 * first]],
        "w0": [w[:, :first]], "w1": [w[:, first:2 * first]], "w2": [w[:, 2 * first:]],
        "vg2": [v[:, 2 * first:], g[:, 2 * first:]],
    }
    packed = jnp.concatenate(
        [part.astype(jnp.bfloat16) for item in plan for part in pieces[item[0]]], axis=1
    )
    sizes = (line, rows, tok_rows, mix_cols, ffn_cols, 2 * tok_cols, mix_kernel.shape[0], ffn_value_kernel.shape[0])
    vm = pltpu.VMEM
    f32, bf16 = jnp.float32, jnp.bfloat16
    lead = -(-(mix_kernel.shape[0] // 2) // 8) * 8
    seqs = tok_rows // SEQ_LEN
    full = (tok_rows, tok_cols)
    scratch = [vm((line, 2, 2, rows, item[2]), bf16) for item in plan] + [
        vm(full, bf16), vm((2,) + full, bf16), vm((tok_rows, mix_cols), f32),
        vm((seqs, SEQ_LEN + 2 * lead, mix_cols), f32), vm((tok_rows, mix_cols), f32),
        vm((tok_rows, 128), f32), vm((tok_rows, 128), f32), vm((tok_rows, mix_cols), bf16),
        vm(full, f32), vm(full, f32), vm(full, f32), vm(full, bf16), vm(full, bf16),
        vm((tok_rows, first), bf16), vm((tok_rows, first), bf16), vm((tok_rows, rest), bf16),
        vm(full, f32), vm(full, f32), vm(full, f32),
        pltpu.SemaphoreType.DMA((len(transfers),)), pltpu.SemaphoreType.DMA((len(transfers),)),
        pltpu.SemaphoreType.DMA((len(plan),)), pltpu.SemaphoreType.DMA((5,)), pltpu.SemaphoreType.DMA((5,)),
    ]
    return pl.pallas_call(
        functools.partial(layer_kernel, sizes, plan, transfers, program),
        out_shape=jax.ShapeDtypeStruct(full, bf16),
        in_specs=[pl.BlockSpec(memory_space=vm)] * 9,
        out_specs=pl.BlockSpec(memory_space=vm),
        scratch_shapes=scratch,
        compiler_params=pltpu.CompilerParams(
            collective_id=0, has_side_effects=True, vmem_limit_bytes=56 * 1024 * 1024
        ),
    )(
        tokens, mix_gain.reshape(2, 1, tok_cols), mix_kernel, chan_gain.reshape(1, -1), chan_bias.reshape(1, -1),
        ffn_gain.reshape(2, 1, tok_cols), ffn_value_kernel, ffn_gate_kernel, packed,
    )


def pick_body(fs_size, tp_size):
    def run(*args):
        tokens, mix_w, ffn_w = args[0], args[2], args[9]
        fits = (
            tp_size == 2 and fs_size % 8 == 0 and fs_size <= 32
            and mix_w.shape[0] % 16 == 0 and mix_w.shape[1] % 256 == 0
            and ffn_w.shape[1] % 256 == 0 and ffn_w.shape[1] >= 768
            and tokens.shape[0] % 64 == 0 and tokens.shape[1] % 128 == 0
            and fs_size * mix_w.shape[0] == tp_size * tokens.shape[1]
            and fs_size * args[7].shape[1] == tp_size * tokens.shape[1]
        )
        if fits:
            return fused_body(fs_size, *args)
        return body(*args)

    return run


def solution(mesh):
    return jax.shard_map(
        pick_body(mesh.shape["fs"], mesh.shape["tp"]),
        mesh=mesh,
        in_specs=(
            P("fs", "tp"),
            P(),
            P("fs", "tp"),
            P("fs", "tp"),
            P(None, "tp"),
            P("tp"),
            P("tp"),
            P("tp", "fs"),
            P(),
            P("fs", "tp"),
            P("fs", "tp"),
            P(None, "tp"),
            P(None, "tp"),
            P("tp", "fs"),
        ),
        out_specs=P("fs", "tp"),
        check_vma=False,
    )
```

```python
import functools

import jax
import jax.numpy as jnp
from jax import lax
from jax.experimental import pallas as pl
from jax.experimental.pallas import tpu as pltpu
from jax.sharding import PartitionSpec as P

CONV_W = 1024
SEQ_LEN = 32


EPS = 1e-06


def rms_rows(act_rows, norm_gain):
    values = act_rows.astype(jnp.float32)
    scaled = values * lax.rsqrt(jnp.mean(values * values, axis=-1, keepdims=True) + EPS)
    return (scaled * norm_gain).astype(jnp.bfloat16)


def along_positions(values, kernel, length):
    seq_count = values.shape[0] // length
    blocks = values.reshape(seq_count, length, values.shape[1])
    half_width = kernel.shape[0] // 2
    padded = jnp.pad(blocks, ((0, 0), (half_width, half_width), (0, 0)))
    summed = jnp.zeros_like(blocks)
    for offset in range(kernel.shape[0]):
        summed = summed + padded[:, offset : offset + length, :] * kernel[offset]
    return summed.reshape(values.shape)


def collect_rows(local_rows):
    return lax.all_gather(local_rows, "tp", axis=1, tiled=True)


def project_in(normed, weight_one, weight_two):
    empty = jnp.zeros((normed.shape[0], weight_one.shape[1]), jnp.float32)

    def add_both(totals, pieces):
        columns = lax.slice_in_dim(normed, 0, pieces[0].shape[0], axis=1)
        first = totals[0] + jnp.dot(
            columns, pieces[0].astype(jnp.bfloat16), preferred_element_type=jnp.float32
        )
        second = totals[1] + jnp.dot(
            columns, pieces[1].astype(jnp.bfloat16), preferred_element_type=jnp.float32
        )
        return (first, second)

    return add_both(
        (empty, empty),
        (
            lax.all_gather(weight_one.astype(jnp.bfloat16), "fs", axis=0, tiled=True),
            lax.all_gather(weight_two.astype(jnp.bfloat16), "fs", axis=0, tiled=True),
        ),
    )


def project_out(active, weight):

    def apply_piece(piece):
        return jnp.dot(active, piece.astype(jnp.bfloat16), preferred_element_type=jnp.float32)

    partial_terms = apply_piece(lax.all_gather(weight.astype(jnp.bfloat16), "fs", axis=1, tiled=True))
    return lax.psum_scatter(partial_terms, "tp", scatter_dimension=1, tiled=True)


def body(
    tokens,
    mix_gain,
    mix_value_w,
    mix_gate_w,
    mix_kernel,
    chan_gain,
    chan_bias,
    mix_out_w,
    ffn_gain,
    ffn_value_w,
    ffn_gate_w,
    ffn_value_kernel,
    ffn_gate_kernel,
    ffn_down_w,
):
    normed = rms_rows(collect_rows(tokens), mix_gain)
    mix_value, mix_gate = project_in(normed, mix_value_w, mix_gate_w)
    glu_rows = mix_value * jax.nn.sigmoid(mix_gate)
    mixed = along_positions(glu_rows, mix_kernel, SEQ_LEN)
    chan_sum, chan_square = lax.psum(
        (jnp.sum(mixed, axis=-1), jnp.sum(mixed * mixed, axis=-1)), "tp"
    )
    chan_mean = (chan_sum / CONV_W)[:, None]
    chan_var = jnp.maximum((chan_square / CONV_W)[:, None] - chan_mean * chan_mean, 0.0)
    active = jax.nn.silu(
        (mixed - chan_mean) * lax.rsqrt(chan_var + EPS) * chan_gain + chan_bias
    ).astype(jnp.bfloat16)
    middle = (tokens.astype(jnp.float32) + project_out(active, mix_out_w)).astype(jnp.bfloat16)
    normed_ffn = rms_rows(collect_rows(middle), ffn_gain)
    up_value, up_gate = project_in(normed_ffn, ffn_value_w, ffn_gate_w)
    up_value = along_positions(up_value, ffn_value_kernel, SEQ_LEN)
    up_gate = along_positions(up_gate, ffn_gate_kernel, SEQ_LEN)
    hidden = (jax.nn.silu(up_gate) * up_value).astype(jnp.bfloat16)
    return (middle.astype(jnp.float32) + project_out(hidden, ffn_down_w)).astype(jnp.bfloat16)


MESH = pl.DeviceIdType.MESH
UNIT_US = 0.36
HOP_US = 1.8


def chunk_plan(mix_cols, ffn_cols):
    wide = (2 * ffn_cols // 5) // 128 * 128
    rest = ffn_cols - 2 * wide
    plan = [
        ("mv", "A", mix_cols), ("mg", "A", mix_cols), ("mo", "A", mix_cols),
        ("vg0", "A", 2 * wide), ("vg1", "A", 2 * wide), ("vg2", "A", 2 * rest),
        ("w0", "A", wide), ("w1", "B", wide), ("w2", "B", rest),
    ]
    gates = {
        "vg1": ("vg0", "u", 1), "vg2": ("vg1", "u", 1), "w0": ("vg1", "u", 2),
        "w1": ("vg2", "u", 2), "w2": ("w0", "u", 2),
    }
    return plan, gates, (wide, wide, rest)


def build_transfers(plan, gates, line):
    out = {}
    steps = range(1, line)
    for name, kind, cols in plan:
        out[(name, "1")] = dict(link="x", size=cols // 128, deps=[], phase="p1")
    for name, kind, cols in plan:
        width = cols // 128
        gate = [gates[name]] if name in gates else []
        if kind == "A":
            for t in steps:
                for d in "ud":
                    deps = [(name, d, t - 1)] if t > 1 else [(name, "1")] + gate
                    out[(name, d, t)] = dict(link="z" + d, size=2 * width, deps=deps, phase="z")
            out[(name, "y", "o", 0)] = dict(link="y", size=2 * width, deps=[(name, "1")], phase="y")
            for t in steps:
                for d in "ud":
                    out[(name, "y", d, t)] = dict(link="y", size=2 * width, deps=[(name, d, t)], phase="y")
        else:
            out[(name, "y", "o", 0)] = dict(link="y", size=2 * width, deps=[(name, "1")], phase="y")
            for t in steps:
                for d in "ud":
                    deps = [(name, d, t - 1)] if t > 1 else [(name, "y", "o", 0)] + gate
                    out[(name, d, t)] = dict(link="z" + d, size=4 * width, deps=deps, phase="q")
    return out


def order_events(transfers, computes):
    free, arrival, seen, done = {}, {}, set(), {}
    program, now = [], 0.0

    def issue():
        for key, item in transfers.items():
            if key not in arrival and all(dep in seen for dep in item["deps"]):
                start = max(now, free.get(item["link"], 0.0))
                free[item["link"]] = start + item["size"] * UNIT_US
                arrival[key] = free[item["link"]] + HOP_US
                program.append(("send", key))
                if key == ("mo", "1"):
                    program.append(("compute", "tok_start"))
                    free["x"] += 5.6

    issue()
    program.append(("local", None))
    while len(seen) < len(transfers) or len(done) < len(computes):
        events = [(arrival[key], i, key) for i, key in enumerate(transfers) if key in arrival and key not in seen]
        ready = []
        for i, (name, needs, after, cost, delay) in enumerate(computes):
            if name in done or not all(a in done for a in after):
                continue
            if all(key in seen for key in transfers if key[0] in needs):
                ready.append((max([delay] + [done[a] + delay for a in after]), i, name, cost))
        can = [r for r in ready if r[0] <= now]
        if events and min(events)[0] <= now:
            pick = min(events)
        elif can:
            pick = min(can, key=lambda r: r[1])
        else:
            pick = min(events + ready, key=lambda r: r[0])
            now = max(now, pick[0])
        if len(pick) == 3:
            seen.add(pick[2])
            program.append(("recv", pick[2]))
            issue()
        else:
            program.append(("compute", pick[2]))
            now += pick[3]
            done[pick[2]] = now
    return program


def compute_list():
    items = [
        ("tok_fwd", (), (), 0.2, 10.0),
        ("norm1", (), ("tok_fwd",), 2.0, 1.5),
        ("mixv", ("mv",), ("norm1",), 0.8, 0.0),
        ("mixg", ("mg",), ("mixv",), 1.0, 0.0),
        ("conv_a", (), ("mixg",), 1.2, 0.0),
        ("conv_b", (), ("conv_a",), 1.2, 0.0),
        ("stats", (), ("conv_b",), 0.7, 0.0),
        ("active", (), ("stats",), 1.5, 2.5),
        ("out_far", ("mo",), ("active",), 0.8, 0.0),
        ("out_near", (), ("out_far",), 0.8, 0.0),
        ("out_x", (), ("out_near",), 0.5, 0.8),
        ("middle", (), ("out_x",), 0.8, 8.0),
        ("mid_fwd", (), ("middle",), 0.2, 8.0),
        ("norm2", (), ("mid_fwd",), 2.0, 1.5),
    ]
    for g in (0, 1, 2):
        items.append(("up%d" % g, ("vg%d" % g,), ("norm2",), (2.0, 2.0, 1.0)[g], 0.0))
    for g in (0, 1, 2):
        items.append(("down_far%d" % g, ("w%d" % g,), ("up%d" % g,), 0.5, 0.0))
    items.append(("send_far", (), tuple("down_far%d" % g for g in (0, 1, 2)), 0.1, 0.0))
    for g in (0, 1, 2):
        items.append(("down_near%d" % g, (), ("send_far", ), 0.5, 0.0))
    items.append(("down_x", (), tuple("down_near%d" % g for g in (0, 1, 2)), 0.5, 0.0))
    items.append(("finish", (), ("down_x",), 1.0, 7.5))
    return items


def layer_kernel(sizes, plan, groups, transfers, program, *refs):
    line, tok_rows, tok_cols, mix_cols, ffn_cols, taps, ffn_taps, total_cols = sizes
    (tokens, gain1, kern, cgain, cbias, gain2, vkern, gkern, packed) = refs[:9]
    out = refs[9]
    scratch = refs[10:]
    held = {item[0]: scratch[i] for i, item in enumerate(plan)}
    (tokall, midall, normed, mvbuf, pad, mixed, stat, stats_in, active,
     far_peer, far_mine, far_in, near_peer, near_mine, near_in, x_out, x_in,
     hid0, hid1, hid2, down_far_peer, down_far_mine, down_far_in,
     down_near_peer, down_near_mine, down_near_in, down_x_out, down_x_in,
     send_sem, recv_sem, loc_sem, act_send, act_recv) = scratch[len(plan):]
    hidden = (hid0, hid1, hid2)
    width = 2 * tok_cols
    offsets, at = {}, 0
    for name, _, cols in plan:
        offsets[name] = at
        at += cols
    cols_of = {item[0]: item[2] for item in plan}
    numbers = {key: i for i, key in enumerate(transfers)}
    fs = lax.axis_index("fs")
    core = lax.axis_index("tp")
    peer = 1 - core
    z, y, x = lax.div(fs, 4), lax.rem(lax.div(fs, 2), 2), lax.rem(fs, 2)
    far = 1 - x
    at_y, at_x = fs + 2 - 4 * y, fs + 1 - 2 * x
    half = line // 2

    barrier = pltpu.get_barrier_semaphore()
    for dev in ({"fs": at_y}, {"fs": at_x}, {"tp": peer}, {"fs": at_x, "tp": peer}):
        pl.semaphore_signal(barrier, inc=1, device_id=dev, device_id_type=MESH)

    @pl.when(z > 0)
    def _():
        pl.semaphore_signal(barrier, inc=1, device_id={"fs": fs - 4}, device_id_type=MESH)

    @pl.when(z < line - 1)
    def _():
        pl.semaphore_signal(barrier, inc=1, device_id={"fs": fs + 4}, device_id_type=MESH)

    def piece(name, part):
        lanes = pl.ds(pl.multiple_of(part * total_cols + offsets[name], 128), cols_of[name])
        return packed.at[:, lanes]

    local = []
    for i, (name, _, cols) in enumerate(plan):
        local.append(pltpu.make_async_copy(piece(name, x), held[name].at[z, y, x], loc_sem.at[i]))
    local.append(pltpu.make_async_copy(tokens, tokall.at[x, core], loc_sem.at[len(plan)]))
    for copy in local:
        copy.start()
    pl.semaphore_wait(barrier, 4 + jnp.minimum(z, 1) + jnp.minimum(line - 1 - z, 1))

    def guards(key, sending):
        phase = transfers[key]["phase"]
        if phase in ("z", "q"):
            d, t = key[1], key[2]
            if d == "u":
                return jnp.logical_and(z >= t - 1, z < line - 1) if sending else z >= t
            return jnp.logical_and(z <= line - t, z > 0) if sending else z <= line - 1 - t
        if phase == "y" and key[2] != "o":
            d, t = key[2], key[3]
            return z >= t if d == "u" else z <= line - 1 - t
        return None

    def make(key, sending):
        phase, name, i = transfers[key]["phase"], key[0], numbers[key]
        buf = held[name]
        src = None
        if phase in ("z", "q"):
            d, t = key[1], key[2]
            back = t - 1 if sending else t
            block = z - back if d == "u" else z + back
            dev = {"fs": fs + 4 if d == "u" else fs - 4}
            dst = buf.at[block, y] if phase == "z" else buf.at[block]
        elif phase == "y":
            d, t = key[2], key[3]
            block = z + t if d == "d" else z - t
            dev = {"fs": at_y}
            dst = buf.at[block, y if sending else 1 - y]
        else:
            dev = {"fs": at_x}
            dst = buf.at[z, y, x if sending else far]
            if sending:
                src = piece(name, far)
        return pltpu.make_async_remote_copy(
            src_ref=dst if src is None else src, dst_ref=dst, send_sem=send_sem.at[i],
            recv_sem=recv_sem.at[i], device_id=dev, device_id_type=MESH,
        )

    def act(key, sending, what):
        guard = guards(key, sending)

        def run():
            what(make(key, sending))

        if guard is None:
            run()
        else:
            pl.when(guard)(run)

    acts = []

    def exchange(src, dst, landed, **dev):
        i = len(acts)
        acts.append(None)

        def build(s, d):
            return pltpu.make_async_remote_copy(
                src_ref=s, dst_ref=d, send_sem=act_send.at[i], recv_sem=act_recv.at[i],
                device_id=dev, device_id_type=MESH,
            )

        acts[i] = build(src, dst)
        return build(src, dst).start, build(landed, landed).wait_recv

    tok_core = exchange(tokens, tokall.at[x, core], tokall.at[x, peer], tp=peer)
    tok_x = exchange(tokens, tokall.at[x, core], tokall.at[far, core], fs=at_x)
    tok_fwd = exchange(tokall.at[far, core], tokall.at[far, core], tokall.at[far, peer], tp=peer)
    mid_core = exchange(midall.at[x, core], midall.at[x, core], midall.at[x, peer], tp=peer)
    mid_x = exchange(midall.at[x, core], midall.at[x, core], midall.at[far, core], fs=at_x)
    mid_fwd = exchange(midall.at[far, core], midall.at[far, core], midall.at[far, peer], tp=peer)
    stat_all = [
        exchange(stat, stats_in.at[0], stats_in.at[0], tp=peer),
        exchange(stat, stats_in.at[1], stats_in.at[1], fs=at_x),
        exchange(stat, stats_in.at[2], stats_in.at[2], fs=at_x, tp=peer),
    ]
    out_far = exchange(far_peer, far_in, far_in, tp=peer)
    out_near = exchange(near_peer, near_in, near_in, tp=peer)
    out_x = exchange(x_out, x_in, x_in, fs=at_x)
    down_far = exchange(down_far_peer, down_far_in, down_far_in, tp=peer)
    down_near = exchange(down_near_peer, down_near_in, down_near_in, tp=peer)
    down_x = exchange(down_x_out, down_x_in, down_x_in, fs=at_x)

    def norm_rows(rows_of, gain):
        for side in (0, 1):
            def block(r, carry):
                at_rows = pl.ds(pl.multiple_of(r * 32, 32), 32)
                a = rows_of[side, 0, at_rows, :].astype(jnp.float32)
                b = rows_of[side, 1, at_rows, :].astype(jnp.float32)
                total = jnp.sum(a * a + b * b, axis=-1, keepdims=True)
                scale = lax.rsqrt(total / width + EPS)
                normed[0, side, at_rows, :] = (a * scale * gain[0]).astype(jnp.bfloat16)
                normed[1, side, at_rows, :] = (b * scale * gain[1]).astype(jnp.bfloat16)
                return carry

            lax.fori_loop(0, tok_rows // 32, block, 0)

    def project(name, lo, hi):
        total = None
        for h in (0, 1):
            weight = held[name][h * half:(h + 1) * half, :, :, :, lo:hi]
            weight = weight.reshape(-1, hi - lo)
            left = normed[h].reshape(2 * tok_rows, tok_cols)
            term = jnp.dot(left, weight, preferred_element_type=jnp.float32)
            total = term if total is None else total + term
        return total

    def project_back(left, name, side):
        weight = held[name][pl.ds(side * half, half)]
        weight = weight.reshape(-1, weight.shape[-1])
        return lax.dot_general(left, weight, (((1,), (1,)), ((), ())), preferred_element_type=jnp.float32)

    def start_tokens():
        tok_core[0]()
        tok_x[0]()

    def forward_tokens():
        tok_x[1]()
        tok_fwd[0]()

    def norm1():
        pad[...] = jnp.zeros_like(pad)
        tok_core[1]()
        tok_fwd[1]()
        norm_rows(tokall, gain1)

    seqs = 2 * tok_rows // SEQ_LEN
    lead = -(-(taps // 2) // 8) * 8

    def mixv():
        mvbuf[...] = project("mv", 0, mix_cols)

    def mixg():
        glu = mvbuf[...] * jax.nn.sigmoid(project("mg", 0, mix_cols))
        pad[:, lead:lead + SEQ_LEN, :] = glu.reshape(seqs, SEQ_LEN, mix_cols)

    lane_blocks = mix_cols // 128

    def conv(lo, hi):
        def block(i, carry):
            s, c = lo + lax.div(i, lane_blocks), lax.rem(i, lane_blocks)
            lanes = pl.ds(pl.multiple_of(c * 128, 128), 128)
            taps_at = pl.ds(pl.multiple_of(x * mix_cols + c * 128, 128), 128)
            total = jnp.zeros((SEQ_LEN, 128), jnp.float32)
            for k in range(taps):
                total = total + pad[s, pl.ds(lead - taps // 2 + k, SEQ_LEN), lanes] * kern[k:k + 1, taps_at]
            mixed[pl.ds(pl.multiple_of(s * SEQ_LEN, SEQ_LEN), SEQ_LEN), lanes] = total
            return carry

        lax.fori_loop(0, (hi - lo) * lane_blocks, block, 0)

    def stats():
        for r in range(0, 2 * tok_rows, 128):
            v = mixed[r:r + 128, :]
            first = jnp.sum(v, axis=-1, keepdims=True)
            second = jnp.sum(v * v, axis=-1, keepdims=True)
            lane = lax.broadcasted_iota(jnp.int32, (128, 128), 1)
            stat[:, r:r + 128] = jnp.where(lane == 0, first, second).T[:8]
        for send, _ in stat_all:
            send()

    def make_active():
        for _, wait in stat_all:
            wait()
        for r in range(0, 2 * tok_rows, 128):
            both = stat[:, r:r + 128] + stats_in[0, :, r:r + 128] + (
                stats_in[1, :, r:r + 128] + stats_in[2, :, r:r + 128]
            )
            both = jnp.concatenate([both] * 16, axis=0).T
            mean = both[:, 0:1] / (4 * mix_cols)
            var = jnp.maximum(both[:, 1:2] / (4 * mix_cols) - mean * mean, 0.0)
            v = (mixed[r:r + 128, :] - mean) * lax.rsqrt(var + EPS) * cgain[x] + cbias[x]
            active[r:r + 128, :] = (v * jax.nn.sigmoid(v)).astype(jnp.bfloat16)

    def rows_at(side):
        return pl.ds(pl.multiple_of(side * tok_rows, tok_rows), tok_rows)

    def make_out_far():
        left = active[rows_at(far), :]
        far_peer[...] = project_back(left, "mo", peer)
        out_far[0]()
        far_mine[...] = project_back(left, "mo", core)

    def make_out_near():
        left = active[rows_at(x), :]
        near_peer[...] = project_back(left, "mo", peer)
        out_far[1]()
        x_out[...] = (far_mine[...] + far_in[...]).astype(jnp.bfloat16)
        out_x[0]()
        out_near[0]()
        near_mine[...] = project_back(left, "mo", core)

    def make_out_x():
        out_near[1]()
        near_mine[...] += near_in[...]

    def make_middle():
        out_x[1]()
        total = tokens[...].astype(jnp.float32) + (near_mine[...] + x_in[...].astype(jnp.float32))
        midall[x, core] = total.astype(jnp.bfloat16)
        mid_x[0]()
        mid_core[0]()

    def forward_middle():
        mid_x[1]()
        mid_fwd[0]()

    def norm2():
        mid_core[1]()
        mid_fwd[1]()
        norm_rows(midall, gain2)

    def short_conv(values, kernel_rows, lanes):
        pos = lax.rem(lax.broadcasted_iota(jnp.int32, values.shape, 0), SEQ_LEN)
        total = None
        for k in range(ffn_taps):
            shift = k - ffn_taps // 2
            term = values
            if shift:
                term = pltpu.roll(values, (-shift) % (2 * tok_rows), 0)
                inside = pos < SEQ_LEN - shift if shift > 0 else pos >= -shift
                term = jnp.where(inside, term, 0.0)
            term = term * kernel_rows[k:k + 1, lanes]
            total = term if total is None else total + term
        return total

    def up(g):
        count = groups[g]
        start = sum(groups[:g])
        for c in range(0, count, 256):
            n = min(256, count - c)
            lanes = pl.ds(pl.multiple_of(x * ffn_cols + start + c, 128), n)
            name = "vg%d" % g
            value = short_conv(project(name, c, c + n), vkern, lanes)
            gate = short_conv(project(name, count + c, count + c + n), gkern, lanes)
            hidden[g][:, c:c + n] = (gate * jax.nn.sigmoid(gate) * value).astype(jnp.bfloat16)

    fresh = set()

    def down(g, where, name, peer_buf, mine_buf):
        left = hidden[g][rows_at(where), :]
        for side, buf in ((peer, peer_buf), (core, mine_buf)):
            term = project_back(left, "w%d" % g, side)
            if name in fresh:
                buf[...] += term
            else:
                buf[...] = term
        fresh.add(name)

    def make_down_x():
        down_near[0]()
        down_far[1]()
        down_x_out[...] = (down_far_mine[...] + down_far_in[...]).astype(jnp.bfloat16)
        down_x[0]()

    def finish():
        down_near[1]()
        near = down_near_mine[...] + down_near_in[...] + midall[x, core].astype(jnp.float32)
        down_near_mine[...] = near
        down_x[1]()
        out[...] = (down_near_mine[...] + down_x_in[...].astype(jnp.float32)).astype(jnp.bfloat16)

    run = {
        "tok_start": start_tokens, "tok_fwd": forward_tokens, "norm1": norm1, "mixv": mixv, "mixg": mixg,
        "conv_a": lambda: conv(0, seqs // 2), "conv_b": lambda: conv(seqs // 2, seqs),
        "stats": stats, "active": make_active, "out_far": make_out_far, "out_near": make_out_near,
        "out_x": make_out_x, "middle": make_middle, "mid_fwd": forward_middle, "norm2": norm2,
        "send_far": down_far[0], "down_x": make_down_x, "finish": finish,
    }
    for g in (0, 1, 2):
        run["up%d" % g] = functools.partial(up, g)
        run["down_far%d" % g] = functools.partial(down, g, far, "far", down_far_peer, down_far_mine)
        run["down_near%d" % g] = functools.partial(down, g, x, "near", down_near_peer, down_near_mine)

    for kind, key in program:
        if kind == "send":
            act(key, True, lambda copy: copy.start())
        elif kind == "recv":
            act(key, False, lambda copy: copy.wait_recv())
        elif kind == "local":
            for copy in local:
                copy.wait()
        else:
            run[key]()
    for key in transfers:
        act(key, True, lambda copy: copy.wait_send())
    for copy in acts:
        copy.wait_send()


def fused_body(fs_size, tokens, mix_gain, mix_value_w, mix_gate_w, mix_kernel, chan_gain, chan_bias, mix_out_w,
               ffn_gain, ffn_value_w, ffn_gate_w, ffn_value_kernel, ffn_gate_kernel, ffn_down_w):
    rows, mix_cols = mix_value_w.shape[0], mix_value_w.shape[1] // 2
    ffn_cols = ffn_value_w.shape[1] // 2
    tok_rows, tok_cols = tokens.shape
    line = fs_size // 4
    plan, gates, groups = chunk_plan(mix_cols, ffn_cols)
    transfers = build_transfers(plan, gates, line)
    program = order_events(transfers, compute_list())
    bf16, f32 = jnp.bfloat16, jnp.float32
    parts = []
    for q in (0, 1):
        for weight in (mix_value_w, mix_gate_w, mix_out_w.T):
            parts.append(weight[:, q * mix_cols:(q + 1) * mix_cols])
        cuts = [q * ffn_cols + sum(groups[:g]) for g in (0, 1, 2)]
        for g in (0, 1, 2):
            for weight in (ffn_value_w, ffn_gate_w):
                parts.append(weight[:, cuts[g]:cuts[g] + groups[g]])
        parts.append(ffn_down_w.T[:, q * ffn_cols:(q + 1) * ffn_cols])
    packed = jnp.concatenate([part.astype(bf16) for part in parts], axis=1)
    sizes = (line, tok_rows, tok_cols, mix_cols, ffn_cols, mix_kernel.shape[0], ffn_value_kernel.shape[0],
             packed.shape[1] // 2)
    vm = pltpu.VMEM
    lead = -(-(mix_kernel.shape[0] // 2) // 8) * 8
    both = 2 * tok_rows
    full = (tok_rows, tok_cols)
    sums = [vm(full, f32)] * 6 + [vm(full, bf16)] * 2
    scratch = [vm((line, 2, 2, rows, item[2]), bf16) for item in plan] + [
        vm((2, 2) + full, bf16), vm((2, 2) + full, bf16), vm((2, 2) + full, bf16),
        vm((both, mix_cols), f32), vm((both // SEQ_LEN, SEQ_LEN + 2 * lead, mix_cols), f32),
        vm((both, mix_cols), f32), vm((8, both), f32), vm((3, 8, both), f32), vm((both, mix_cols), bf16),
    ] + sums + [vm((both, g), bf16) for g in groups] + sums + [
        pltpu.SemaphoreType.DMA((len(transfers),)), pltpu.SemaphoreType.DMA((len(transfers),)),
        pltpu.SemaphoreType.DMA((len(plan) + 1,)), pltpu.SemaphoreType.DMA((15,)), pltpu.SemaphoreType.DMA((15,)),
    ]
    return pl.pallas_call(
        functools.partial(layer_kernel, sizes, plan, groups, transfers, program),
        out_shape=jax.ShapeDtypeStruct(full, bf16),
        in_specs=[pl.BlockSpec(memory_space=vm)] * 9,
        out_specs=pl.BlockSpec(memory_space=vm),
        scratch_shapes=scratch,
        compiler_params=pltpu.CompilerParams(
            collective_id=0, has_side_effects=True, vmem_limit_bytes=56 * 1024 * 1024
        ),
    )(
        tokens, mix_gain.reshape(2, 1, tok_cols), mix_kernel, chan_gain.reshape(2, 1, -1),
        chan_bias.reshape(2, 1, -1), ffn_gain.reshape(2, 1, tok_cols), ffn_value_kernel, ffn_gate_kernel, packed,
    )


def pick_body(fs_size, tp_size):
    def run(*args):
        tokens, mix_w, ffn_w = args[0], args[2], args[9]
        fits = (
            tp_size == 2 and fs_size % 8 == 0 and fs_size <= 32
            and mix_w.shape[0] % 16 == 0 and mix_w.shape[1] % 256 == 0
            and ffn_w.shape[1] % 256 == 0 and ffn_w.shape[1] >= 1024
            and tokens.shape[0] % 64 == 0 and tokens.shape[1] % 128 == 0
            and fs_size * mix_w.shape[0] == tp_size * tokens.shape[1]
            and fs_size * args[7].shape[1] == tp_size * tokens.shape[1]
        )
        if fits:
            return fused_body(fs_size, *args)
        return body(*args)

    return run


def solution(mesh):
    return jax.shard_map(
        pick_body(mesh.shape["fs"], mesh.shape["tp"]),
        mesh=mesh,
        in_specs=(
            P("fs", "tp"),
            P(),
            P("fs", "tp"),
            P("fs", "tp"),
            P(None, "tp"),
            P("tp"),
            P("tp"),
            P("tp", "fs"),
            P(),
            P("fs", "tp"),
            P("fs", "tp"),
            P(None, "tp"),
            P(None, "tp"),
            P("tp", "fs"),
        ),
        out_specs=P("fs", "tp"),
        check_vma=False,
    )
```

```python
import functools

import jax
import jax.numpy as jnp
from jax import lax
from jax.experimental import pallas as pl
from jax.experimental.pallas import tpu as pltpu
from jax.sharding import PartitionSpec as P

CONV_W = 1024
SEQ_LEN = 32


EPS = 1e-06


def rms_rows(act_rows, norm_gain):
    values = act_rows.astype(jnp.float32)
    scaled = values * lax.rsqrt(jnp.mean(values * values, axis=-1, keepdims=True) + EPS)
    return (scaled * norm_gain).astype(jnp.bfloat16)


def along_positions(values, kernel, length):
    seq_count = values.shape[0] // length
    blocks = values.reshape(seq_count, length, values.shape[1])
    half_width = kernel.shape[0] // 2
    padded = jnp.pad(blocks, ((0, 0), (half_width, half_width), (0, 0)))
    summed = jnp.zeros_like(blocks)
    for offset in range(kernel.shape[0]):
        summed = summed + padded[:, offset : offset + length, :] * kernel[offset]
    return summed.reshape(values.shape)


def collect_rows(local_rows):
    return lax.all_gather(local_rows, "tp", axis=1, tiled=True)


def project_in(normed, weight_one, weight_two):
    empty = jnp.zeros((normed.shape[0], weight_one.shape[1]), jnp.float32)

    def add_both(totals, pieces):
        columns = lax.slice_in_dim(normed, 0, pieces[0].shape[0], axis=1)
        first = totals[0] + jnp.dot(
            columns, pieces[0].astype(jnp.bfloat16), preferred_element_type=jnp.float32
        )
        second = totals[1] + jnp.dot(
            columns, pieces[1].astype(jnp.bfloat16), preferred_element_type=jnp.float32
        )
        return (first, second)

    return add_both(
        (empty, empty),
        (
            lax.all_gather(weight_one.astype(jnp.bfloat16), "fs", axis=0, tiled=True),
            lax.all_gather(weight_two.astype(jnp.bfloat16), "fs", axis=0, tiled=True),
        ),
    )


def project_out(active, weight):

    def apply_piece(piece):
        return jnp.dot(active, piece.astype(jnp.bfloat16), preferred_element_type=jnp.float32)

    partial_terms = apply_piece(lax.all_gather(weight.astype(jnp.bfloat16), "fs", axis=1, tiled=True))
    return lax.psum_scatter(partial_terms, "tp", scatter_dimension=1, tiled=True)


def body(
    tokens,
    mix_gain,
    mix_value_w,
    mix_gate_w,
    mix_kernel,
    chan_gain,
    chan_bias,
    mix_out_w,
    ffn_gain,
    ffn_value_w,
    ffn_gate_w,
    ffn_value_kernel,
    ffn_gate_kernel,
    ffn_down_w,
):
    normed = rms_rows(collect_rows(tokens), mix_gain)
    mix_value, mix_gate = project_in(normed, mix_value_w, mix_gate_w)
    glu_rows = mix_value * jax.nn.sigmoid(mix_gate)
    mixed = along_positions(glu_rows, mix_kernel, SEQ_LEN)
    chan_sum, chan_square = lax.psum(
        (jnp.sum(mixed, axis=-1), jnp.sum(mixed * mixed, axis=-1)), "tp"
    )
    chan_mean = (chan_sum / CONV_W)[:, None]
    chan_var = jnp.maximum((chan_square / CONV_W)[:, None] - chan_mean * chan_mean, 0.0)
    active = jax.nn.silu(
        (mixed - chan_mean) * lax.rsqrt(chan_var + EPS) * chan_gain + chan_bias
    ).astype(jnp.bfloat16)
    middle = (tokens.astype(jnp.float32) + project_out(active, mix_out_w)).astype(jnp.bfloat16)
    normed_ffn = rms_rows(collect_rows(middle), ffn_gain)
    up_value, up_gate = project_in(normed_ffn, ffn_value_w, ffn_gate_w)
    up_value = along_positions(up_value, ffn_value_kernel, SEQ_LEN)
    up_gate = along_positions(up_gate, ffn_gate_kernel, SEQ_LEN)
    hidden = (jax.nn.silu(up_gate) * up_value).astype(jnp.bfloat16)
    return (middle.astype(jnp.float32) + project_out(hidden, ffn_down_w)).astype(jnp.bfloat16)


MESH = pl.DeviceIdType.MESH
UNIT_US = 0.36
HOP_US = 2.2


def chunk_plan(mix_cols, ffn_cols):
    wide = (2 * ffn_cols // 5) // 128 * 128
    rest = ffn_cols - 2 * wide
    plan = [
        ("mv", "A", mix_cols), ("mg", "A", mix_cols), ("mo", "B", mix_cols),
        ("vg0", "A", 2 * wide), ("vg1", "A", 2 * wide), ("vg2", "A", 2 * rest),
        ("w0", "A", wide), ("w1", "A", wide), ("w2", "B", rest),
    ]
    gates = {
        "vg0": ("mo", "u", 1), "vg1": ("vg0", "u", 1), "vg2": ("vg1", "u", 1), "w0": ("vg2", "u", 1),
        "w1": ("w0", "u", 1), "w2": ("w1", "u", 1),
    }
    return plan, gates, (wide, wide, rest)


def build_transfers(plan, gates, line):
    out = {}
    steps = range(1, line)
    for name, kind, cols in plan:
        out[(name, "1")] = dict(link="x", size=cols // 128, deps=[], phase="p1")
    for name, kind, cols in plan:
        width = cols // 128
        gate = [gates[name]] if name in gates else []
        late = [("mg", d, line - 1) for d in "ud"] if name in gates else []
        if kind == "A":
            for t in steps:
                for d in "ud":
                    deps = [(name, d, t - 1)] if t > 1 else [(name, "1")] + gate
                    out[(name, d, t)] = dict(link="z" + d, size=2 * width, deps=deps, phase="z")
            out[(name, "y", "o", 0)] = dict(link="y", size=2 * width, deps=[(name, "1")] + late, phase="y")
            for t in steps:
                for d in "ud":
                    out[(name, "y", d, t)] = dict(link="y", size=2 * width, deps=[(name, d, t)], phase="y")
        else:
            out[(name, "y", "o", 0)] = dict(link="y", size=2 * width, deps=[(name, "1")] + late, phase="y")
            for t in steps:
                for d in "ud":
                    deps = [(name, d, t - 1)] if t > 1 else [(name, "y", "o", 0)] + gate
                    out[(name, d, t)] = dict(link="z" + d, size=4 * width, deps=deps, phase="q")
    return out


def order_events(transfers, computes):
    free, arrival, seen, done = {}, {}, set(), {}
    program, now = [], 0.0

    def issue():
        for key, item in transfers.items():
            if key not in arrival and all(dep in seen for dep in item["deps"]):
                start = max(now, free.get(item["link"], 0.0))
                share = 0.5 if key[1] == "y" and key[2] != "o" else 1.0
                free[item["link"]] = start + share * item["size"] * UNIT_US
                arrival[key] = free[item["link"]] + HOP_US
                program.append(("send", key))
                if key == ("mo", "1"):
                    program.append(("compute", "tok_start"))
                    free["x"] += 5.6

    issue()
    program.append(("local", None))
    while len(seen) < len(transfers) or len(done) < len(computes):
        events = [(arrival[key], i, key) for i, key in enumerate(transfers) if key in arrival and key not in seen]
        ready = []
        for i, (name, needs, after, cost, delay) in enumerate(computes):
            if name in done or not all(a in done for a in after):
                continue
            if all(key in seen for key in transfers if key[0] in needs):
                ready.append((max([delay] + [done[a] + delay for a in after]), i, name, cost))
        can = [r for r in ready if r[0] <= now]
        if events and min(events)[0] <= now:
            pick = min(events)
        elif can:
            pick = min(can, key=lambda r: r[1])
        else:
            pick = min(events + ready, key=lambda r: r[0])
            now = max(now, pick[0])
        if len(pick) == 3:
            seen.add(pick[2])
            program.append(("recv", pick[2]))
            issue()
        else:
            program.append(("compute", pick[2]))
            now += pick[3]
            done[pick[2]] = now
    return program


def compute_list():
    items = [
        ("norm1_near", (), (), 1.2, 4.0),
        ("tok_fwd", (), (), 0.2, 9.5),
        ("norm1_far", (), ("tok_fwd",), 1.2, 1.2),
        ("mixv", ("mv",), ("norm1_near", "norm1_far"), 0.7, 0.0),
        ("mixg", ("mg",), ("mixv",), 0.7, 0.0),
        ("conv_a", (), ("mixg",), 1.7, 0.0),
        ("conv_b", (), ("conv_a",), 1.7, 0.0),
        ("stats", (), ("conv_b",), 0.4, 0.0),
        ("active_far", (), ("stats",), 0.6, 3.0),
        ("out_far", ("mo",), ("active_far",), 0.6, 0.0),
        ("active_near", (), ("out_far",), 0.6, 0.0),
        ("out_near", (), ("active_near",), 1.0, 0.0),
        ("out_x", (), ("out_near",), 0.4, 0.8),
        ("middle", (), ("out_x",), 0.6, 11.5),
        ("norm2_near", (), ("middle",), 1.2, 1.2),
        ("mid_fwd", (), ("middle",), 0.2, 8.0),
        ("norm2_far", (), ("mid_fwd",), 1.2, 1.2),
    ]
    for side in ("far", "near"):
        for g in (0, 1, 2):
            items.append(("up_%s%d" % (side, g), ("vg%d" % g,), ("norm2_" + side,), (0.8, 0.8, 0.5)[g], 0.0))
        for g in (0, 1, 2):
            items.append(("down_%s%d" % (side, g), ("w%d" % g,), ("up_%s%d" % (side, g),), 0.4, 0.0))
        items.append(("send_" + side, (), tuple("down_%s%d" % (side, g) for g in (0, 1, 2)), 0.1, 0.0))
    items.append(("down_x", (), ("send_far",), 0.5, 1.0))
    items.append(("finish", (), ("down_x", "send_near"), 1.0, 7.5))
    return items


def layer_kernel(sizes, plan, groups, transfers, program, *refs):
    line, tok_rows, tok_cols, mix_cols, ffn_cols, taps, ffn_taps, total_cols = sizes
    (tokens, gain1, kern, cgain, cbias, gain2, vkern, gkern, packed) = refs[:9]
    out = refs[9]
    scratch = refs[10:]
    held = {item[0]: scratch[i] for i, item in enumerate(plan)}
    (tokall, midall, normed, mvbuf, pad, mixed, stat, stats_in, active,
     far_peer, far_mine, far_in, near_peer, near_mine, near_in, x_out, x_in,
     hid0, hid1, hid2, down_far_peer, down_far_mine, down_far_in,
     down_near_peer, down_near_mine, down_near_in, down_x_out, down_x_in,
     send_sem, recv_sem, loc_sem, act_send, act_recv) = scratch[len(plan):]
    hidden = (hid0, hid1, hid2)
    width = 2 * tok_cols
    offsets, at = {}, 0
    for name, _, cols in plan:
        offsets[name] = at
        at += cols
    cols_of = {item[0]: item[2] for item in plan}
    numbers = {key: i for i, key in enumerate(transfers)}
    fs = lax.axis_index("fs")
    core = lax.axis_index("tp")
    peer = 1 - core
    z, y, x = lax.div(fs, 4), lax.rem(lax.div(fs, 2), 2), lax.rem(fs, 2)
    far = 1 - x
    at_y, at_x = fs + 2 - 4 * y, fs + 1 - 2 * x
    half = line // 2

    barrier = pltpu.get_barrier_semaphore()
    for dev in ({"fs": at_y}, {"fs": at_x}, {"tp": peer}, {"fs": at_x, "tp": peer}):
        pl.semaphore_signal(barrier, inc=1, device_id=dev, device_id_type=MESH)

    @pl.when(z > 0)
    def _():
        pl.semaphore_signal(barrier, inc=1, device_id={"fs": fs - 4}, device_id_type=MESH)

    @pl.when(z < line - 1)
    def _():
        pl.semaphore_signal(barrier, inc=1, device_id={"fs": fs + 4}, device_id_type=MESH)

    def piece(name, part):
        lanes = pl.ds(pl.multiple_of(part * total_cols + offsets[name], 128), cols_of[name])
        return packed.at[:, lanes]

    local = []
    for i, (name, _, cols) in enumerate(plan):
        local.append(pltpu.make_async_copy(piece(name, x), held[name].at[z, y, x], loc_sem.at[i]))
    local.append(pltpu.make_async_copy(tokens, tokall.at[x, core], loc_sem.at[len(plan)]))
    for copy in local:
        copy.start()
    pl.semaphore_wait(barrier, 4 + jnp.minimum(z, 1) + jnp.minimum(line - 1 - z, 1))

    def guards(key, sending):
        phase = transfers[key]["phase"]
        if phase in ("z", "q"):
            d, t = key[1], key[2]
            if d == "u":
                return jnp.logical_and(z >= t - 1, z < line - 1) if sending else z >= t
            return jnp.logical_and(z <= line - t, z > 0) if sending else z <= line - 1 - t
        if phase == "y" and key[2] != "o":
            d, t = key[2], key[3]
            return z >= t if d == "u" else z <= line - 1 - t
        return None

    def make(key, sending):
        phase, name, i = transfers[key]["phase"], key[0], numbers[key]
        buf = held[name]
        src = None
        if phase in ("z", "q"):
            d, t = key[1], key[2]
            back = t - 1 if sending else t
            block = z - back if d == "u" else z + back
            dev = {"fs": fs + 4 if d == "u" else fs - 4}
            dst = buf.at[block, y] if phase == "z" else buf.at[block]
        elif phase == "y":
            d, t = key[2], key[3]
            block = z + t if d == "d" else z - t
            dev = {"fs": at_y}
            dst = buf.at[block, y if sending else 1 - y]
        else:
            dev = {"fs": at_x}
            dst = buf.at[z, y, x if sending else far]
            if sending:
                src = piece(name, far)
        return pltpu.make_async_remote_copy(
            src_ref=dst if src is None else src, dst_ref=dst, send_sem=send_sem.at[i],
            recv_sem=recv_sem.at[i], device_id=dev, device_id_type=MESH,
        )

    def act(key, sending, what):
        guard = guards(key, sending)

        def run():
            what(make(key, sending))

        if guard is None:
            run()
        else:
            pl.when(guard)(run)

    acts = []

    def exchange(src, dst, landed, **dev):
        i = len(acts)
        acts.append(None)

        def build(s, d):
            return pltpu.make_async_remote_copy(
                src_ref=s, dst_ref=d, send_sem=act_send.at[i], recv_sem=act_recv.at[i],
                device_id=dev, device_id_type=MESH,
            )

        acts[i] = build(src, dst)
        return build(src, dst).start, build(landed, landed).wait_recv

    tok_core = exchange(tokens, tokall.at[x, core], tokall.at[x, peer], tp=peer)
    tok_x = exchange(tokens, tokall.at[x, core], tokall.at[far, core], fs=at_x)
    tok_fwd = exchange(tokall.at[far, core], tokall.at[far, core], tokall.at[far, peer], tp=peer)
    mid_core = exchange(midall.at[x, core], midall.at[x, core], midall.at[x, peer], tp=peer)
    mid_x = exchange(midall.at[x, core], midall.at[x, core], midall.at[far, core], fs=at_x)
    mid_fwd = exchange(midall.at[far, core], midall.at[far, core], midall.at[far, peer], tp=peer)
    stat_all = [
        exchange(stat, stats_in.at[0], stats_in.at[0], tp=peer),
        exchange(stat, stats_in.at[1], stats_in.at[1], fs=at_x),
        exchange(stat, stats_in.at[2], stats_in.at[2], fs=at_x, tp=peer),
    ]
    out_far = exchange(far_peer, far_in, far_in, tp=peer)
    out_near = exchange(near_peer, near_in, near_in, tp=peer)
    out_x = exchange(x_out, x_in, x_in, fs=at_x)
    down_far = exchange(down_far_peer, down_far_in, down_far_in, tp=peer)
    down_near = exchange(down_near_peer, down_near_in, down_near_in, tp=peer)
    down_x = exchange(down_x_out, down_x_in, down_x_in, fs=at_x)

    def norm_rows(rows_of, gain, side):
        def block(r, carry):
            at_rows = pl.ds(pl.multiple_of(r * 64, 64), 64)
            a = rows_of[side, 0, at_rows, :].astype(jnp.float32)
            b = rows_of[side, 1, at_rows, :].astype(jnp.float32)
            total = jnp.sum(a * a + b * b, axis=-1, keepdims=True)
            scale = lax.rsqrt(total / width + EPS)
            normed[0, side, at_rows, :] = (a * scale * gain[0]).astype(jnp.bfloat16)
            normed[1, side, at_rows, :] = (b * scale * gain[1]).astype(jnp.bfloat16)
            return carry

        lax.fori_loop(0, tok_rows // 64, block, 0)

    def project(name, lo, hi, side=None):
        total = None
        for h in (0, 1):
            weight = held[name][h * half:(h + 1) * half, :, :, :, lo:hi]
            weight = weight.reshape(-1, hi - lo)
            left = normed[h].reshape(2 * tok_rows, tok_cols) if side is None else normed[h, side]
            term = jnp.dot(left, weight, preferred_element_type=jnp.float32)
            total = term if total is None else total + term
        return total

    def project_back(left, name, side):
        weight = held[name][pl.ds(side * half, half)]
        weight = weight.reshape(-1, weight.shape[-1])
        return lax.dot_general(left, weight, (((1,), (1,)), ((), ())), preferred_element_type=jnp.float32)

    def start_tokens():
        tok_core[0]()
        tok_x[0]()

    def forward_tokens():
        tok_x[1]()
        tok_fwd[0]()

    def norm1_near():
        pad[...] = jnp.zeros_like(pad)
        tok_core[1]()
        norm_rows(tokall, gain1, x)

    def norm1_far():
        tok_fwd[1]()
        norm_rows(tokall, gain1, far)

    seqs = 2 * tok_rows // SEQ_LEN
    lead = -(-(taps // 2) // 8) * 8

    def mixv():
        mvbuf[...] = project("mv", 0, mix_cols)

    def mixg():
        glu = mvbuf[...] * jax.nn.sigmoid(project("mg", 0, mix_cols))
        pad[:, lead:lead + SEQ_LEN, :] = glu.reshape(seqs, SEQ_LEN, mix_cols)

    lane_blocks = mix_cols // 128

    def conv(lo, hi):
        def block(i, carry):
            s, c = lo + lax.div(i, lane_blocks), lax.rem(i, lane_blocks)
            lanes = pl.ds(pl.multiple_of(c * 128, 128), 128)
            taps_at = pl.ds(pl.multiple_of(x * mix_cols + c * 128, 128), 128)
            total = jnp.zeros((SEQ_LEN, 128), jnp.float32)
            for k in range(taps):
                total = total + pad[s, pl.ds(lead - taps // 2 + k, SEQ_LEN), lanes] * kern[k:k + 1, taps_at]
            mixed[pl.ds(pl.multiple_of(s * SEQ_LEN, SEQ_LEN), SEQ_LEN), lanes] = total
            return carry

        lax.fori_loop(0, (hi - lo) * lane_blocks, block, 0)

    def stats():
        for r in range(0, 2 * tok_rows, 128):
            v = mixed[r:r + 128, :]
            first = jnp.sum(v, axis=-1, keepdims=True)
            second = jnp.sum(v * v, axis=-1, keepdims=True)
            lane = lax.broadcasted_iota(jnp.int32, (128, 128), 1)
            stat[:, r:r + 128] = jnp.where(lane == 0, first, second).T[:8]
        for send, _ in stat_all:
            send()

    def make_active(side, first):
        if first:
            for _, wait in stat_all:
                wait()
        for r in range(0, tok_rows, 128):
            at_rows = pl.ds(pl.multiple_of(side * tok_rows + r, 128), 128)
            both = stat[:, at_rows] + stats_in[0, :, at_rows] + (stats_in[1, :, at_rows] + stats_in[2, :, at_rows])
            both = jnp.concatenate([both] * 16, axis=0).T
            mean = both[:, 0:1] / (4 * mix_cols)
            var = jnp.maximum(both[:, 1:2] / (4 * mix_cols) - mean * mean, 0.0)
            v = (mixed[at_rows, :] - mean) * lax.rsqrt(var + EPS) * cgain[x] + cbias[x]
            active[at_rows, :] = (v * jax.nn.sigmoid(v)).astype(jnp.bfloat16)

    def rows_at(side):
        return pl.ds(pl.multiple_of(side * tok_rows, tok_rows), tok_rows)

    def make_out_far():
        left = active[rows_at(far), :]
        far_peer[...] = project_back(left, "mo", peer)
        out_far[0]()
        far_mine[...] = project_back(left, "mo", core)

    def make_out_near():
        out_far[1]()
        x_out[...] = far_mine[...] + far_in[...]
        out_x[0]()
        left = active[rows_at(x), :]
        near_peer[...] = project_back(left, "mo", peer)
        out_near[0]()
        near_mine[...] = project_back(left, "mo", core)

    def make_out_x():
        out_near[1]()
        near_mine[...] += near_in[...]

    def make_middle():
        out_x[1]()
        total = tokens[...].astype(jnp.float32) + (near_mine[...] + x_in[...])
        midall[x, core] = total.astype(jnp.bfloat16)
        mid_x[0]()
        mid_core[0]()

    def forward_middle():
        mid_x[1]()
        mid_fwd[0]()

    def norm2_near():
        mid_core[1]()
        norm_rows(midall, gain2, x)

    def norm2_far():
        mid_fwd[1]()
        norm_rows(midall, gain2, far)

    def short_conv(values, kernel_rows, lanes):
        pos = lax.rem(lax.broadcasted_iota(jnp.int32, values.shape, 0), SEQ_LEN)
        total = None
        for k in range(ffn_taps):
            shift = k - ffn_taps // 2
            term = values
            if shift:
                term = pltpu.roll(values, (-shift) % tok_rows, 0)
                inside = pos < SEQ_LEN - shift if shift > 0 else pos >= -shift
                term = jnp.where(inside, term, 0.0)
            term = term * kernel_rows[k:k + 1, lanes]
            total = term if total is None else total + term
        return total

    def up(g, side):
        count = groups[g]
        start = sum(groups[:g])
        for c in range(0, count, 256):
            n = min(256, count - c)
            lanes = pl.ds(pl.multiple_of(x * ffn_cols + start + c, 128), n)
            name = "vg%d" % g
            value = short_conv(project(name, c, c + n, side), vkern, lanes)
            gate = short_conv(project(name, count + c, count + c + n, side), gkern, lanes)
            hidden[g][side, :, c:c + n] = (gate * jax.nn.sigmoid(gate) * value).astype(jnp.bfloat16)

    fresh = set()

    def down(g, where, name, peer_buf, mine_buf):
        left = hidden[g][where]
        for side, buf in ((peer, peer_buf), (core, mine_buf)):
            term = project_back(left, "w%d" % g, side)
            if name in fresh:
                buf[...] += term
            else:
                buf[...] = term
        fresh.add(name)

    def make_down_x():
        down_far[1]()
        down_x_out[...] = (down_far_mine[...] + down_far_in[...]).astype(jnp.bfloat16)
        down_x[0]()

    def finish():
        down_near[1]()
        near = down_near_mine[...] + down_near_in[...] + midall[x, core].astype(jnp.float32)
        down_near_mine[...] = near
        down_x[1]()
        out[...] = (down_near_mine[...] + down_x_in[...].astype(jnp.float32)).astype(jnp.bfloat16)

    run = {
        "tok_start": start_tokens, "tok_fwd": forward_tokens, "norm1_near": norm1_near, "norm1_far": norm1_far,
        "mixv": mixv, "mixg": mixg, "conv_a": lambda: conv(0, seqs // 2), "conv_b": lambda: conv(seqs // 2, seqs),
        "stats": stats, "active_far": lambda: make_active(far, True), "active_near": lambda: make_active(x, False),
        "out_far": make_out_far, "out_near": make_out_near, "out_x": make_out_x, "middle": make_middle,
        "mid_fwd": forward_middle, "norm2_near": norm2_near, "norm2_far": norm2_far,
        "send_far": down_far[0], "send_near": down_near[0], "down_x": make_down_x, "finish": finish,
    }
    for g in (0, 1, 2):
        run["up_far%d" % g] = functools.partial(up, g, far)
        run["up_near%d" % g] = functools.partial(up, g, x)
        run["down_far%d" % g] = functools.partial(down, g, far, "far", down_far_peer, down_far_mine)
        run["down_near%d" % g] = functools.partial(down, g, x, "near", down_near_peer, down_near_mine)

    for kind, key in program:
        if kind == "send":
            act(key, True, lambda copy: copy.start())
        elif kind == "recv":
            act(key, False, lambda copy: copy.wait_recv())
        elif kind == "local":
            for copy in local:
                copy.wait()
        else:
            run[key]()
    for key in transfers:
        act(key, True, lambda copy: copy.wait_send())
    for copy in acts:
        copy.wait_send()


def fused_body(fs_size, tokens, mix_gain, mix_value_w, mix_gate_w, mix_kernel, chan_gain, chan_bias, mix_out_w,
               ffn_gain, ffn_value_w, ffn_gate_w, ffn_value_kernel, ffn_gate_kernel, ffn_down_w):
    rows, mix_cols = mix_value_w.shape[0], mix_value_w.shape[1] // 2
    ffn_cols = ffn_value_w.shape[1] // 2
    tok_rows, tok_cols = tokens.shape
    line = fs_size // 4
    plan, gates, groups = chunk_plan(mix_cols, ffn_cols)
    transfers = build_transfers(plan, gates, line)
    program = order_events(transfers, compute_list())
    bf16, f32 = jnp.bfloat16, jnp.float32
    parts = []
    for q in (0, 1):
        for weight in (mix_value_w, mix_gate_w, mix_out_w.T):
            parts.append(weight[:, q * mix_cols:(q + 1) * mix_cols])
        cuts = [q * ffn_cols + sum(groups[:g]) for g in (0, 1, 2)]
        for g in (0, 1, 2):
            for weight in (ffn_value_w, ffn_gate_w):
                parts.append(weight[:, cuts[g]:cuts[g] + groups[g]])
        parts.append(ffn_down_w.T[:, q * ffn_cols:(q + 1) * ffn_cols])
    packed = jnp.concatenate([part.astype(bf16) for part in parts], axis=1)
    sizes = (line, tok_rows, tok_cols, mix_cols, ffn_cols, mix_kernel.shape[0], ffn_value_kernel.shape[0],
             packed.shape[1] // 2)
    vm = pltpu.VMEM
    lead = -(-(mix_kernel.shape[0] // 2) // 8) * 8
    both = 2 * tok_rows
    full = (tok_rows, tok_cols)
    sums = [vm(full, f32)] * 6
    scratch = [vm((line, 2, 2, rows, item[2]), bf16) for item in plan] + [
        vm((2, 2) + full, bf16), vm((2, 2) + full, bf16), vm((2, 2) + full, bf16),
        vm((both, mix_cols), f32), vm((both // SEQ_LEN, SEQ_LEN + 2 * lead, mix_cols), f32),
        vm((both, mix_cols), f32), vm((8, both), f32), vm((3, 8, both), f32), vm((both, mix_cols), bf16),
    ] + sums + [vm(full, f32)] * 2 + [vm((2, tok_rows, g), bf16) for g in groups] + sums + [vm(full, bf16)] * 2 + [
        pltpu.SemaphoreType.DMA((len(transfers),)), pltpu.SemaphoreType.DMA((len(transfers),)),
        pltpu.SemaphoreType.DMA((len(plan) + 1,)), pltpu.SemaphoreType.DMA((15,)), pltpu.SemaphoreType.DMA((15,)),
    ]
    return pl.pallas_call(
        functools.partial(layer_kernel, sizes, plan, groups, transfers, program),
        out_shape=jax.ShapeDtypeStruct(full, bf16),
        in_specs=[pl.BlockSpec(memory_space=vm)] * 9,
        out_specs=pl.BlockSpec(memory_space=vm),
        scratch_shapes=scratch,
        compiler_params=pltpu.CompilerParams(
            collective_id=0, has_side_effects=True, vmem_limit_bytes=56 * 1024 * 1024
        ),
    )(
        tokens, mix_gain.reshape(2, 1, tok_cols), mix_kernel, chan_gain.reshape(2, 1, -1),
        chan_bias.reshape(2, 1, -1), ffn_gain.reshape(2, 1, tok_cols), ffn_value_kernel, ffn_gate_kernel, packed,
    )


def pick_body(fs_size, tp_size):
    def run(*args):
        tokens, mix_w, ffn_w = args[0], args[2], args[9]
        fits = (
            tp_size == 2 and fs_size % 8 == 0 and fs_size <= 32
            and mix_w.shape[0] % 16 == 0 and mix_w.shape[1] % 256 == 0
            and ffn_w.shape[1] % 256 == 0 and ffn_w.shape[1] >= 1024
            and tokens.shape[0] % 64 == 0 and tokens.shape[1] % 128 == 0
            and fs_size * mix_w.shape[0] == tp_size * tokens.shape[1]
            and fs_size * args[7].shape[1] == tp_size * tokens.shape[1]
        )
        if fits:
            return fused_body(fs_size, *args)
        return body(*args)

    return run


def solution(mesh):
    return jax.shard_map(
        pick_body(mesh.shape["fs"], mesh.shape["tp"]),
        mesh=mesh,
        in_specs=(
            P("fs", "tp"),
            P(),
            P("fs", "tp"),
            P("fs", "tp"),
            P(None, "tp"),
            P("tp"),
            P("tp"),
            P("tp", "fs"),
            P(),
            P("fs", "tp"),
            P("fs", "tp"),
            P(None, "tp"),
            P(None, "tp"),
            P("tp", "fs"),
        ),
        out_specs=P("fs", "tp"),
        check_vma=False,
    )
```

```python
import functools

import jax
import jax.numpy as jnp
from jax import lax
from jax.experimental import pallas as pl
from jax.experimental.pallas import tpu as pltpu
from jax.sharding import PartitionSpec as P

CONV_W = 1024
SEQ_LEN = 32


EPS = 1e-06


def rms_rows(act_rows, norm_gain):
    values = act_rows.astype(jnp.float32)
    scaled = values * lax.rsqrt(jnp.mean(values * values, axis=-1, keepdims=True) + EPS)
    return (scaled * norm_gain).astype(jnp.bfloat16)


def along_positions(values, kernel, length):
    seq_count = values.shape[0] // length
    blocks = values.reshape(seq_count, length, values.shape[1])
    half_width = kernel.shape[0] // 2
    padded = jnp.pad(blocks, ((0, 0), (half_width, half_width), (0, 0)))
    summed = jnp.zeros_like(blocks)
    for offset in range(kernel.shape[0]):
        summed = summed + padded[:, offset : offset + length, :] * kernel[offset]
    return summed.reshape(values.shape)


def collect_rows(local_rows):
    return lax.all_gather(local_rows, "tp", axis=1, tiled=True)


def project_in(normed, weight_one, weight_two):
    empty = jnp.zeros((normed.shape[0], weight_one.shape[1]), jnp.float32)

    def add_both(totals, pieces):
        columns = lax.slice_in_dim(normed, 0, pieces[0].shape[0], axis=1)
        first = totals[0] + jnp.dot(
            columns, pieces[0].astype(jnp.bfloat16), preferred_element_type=jnp.float32
        )
        second = totals[1] + jnp.dot(
            columns, pieces[1].astype(jnp.bfloat16), preferred_element_type=jnp.float32
        )
        return (first, second)

    return add_both(
        (empty, empty),
        (
            lax.all_gather(weight_one.astype(jnp.bfloat16), "fs", axis=0, tiled=True),
            lax.all_gather(weight_two.astype(jnp.bfloat16), "fs", axis=0, tiled=True),
        ),
    )


def project_out(active, weight):

    def apply_piece(piece):
        return jnp.dot(active, piece.astype(jnp.bfloat16), preferred_element_type=jnp.float32)

    partial_terms = apply_piece(lax.all_gather(weight.astype(jnp.bfloat16), "fs", axis=1, tiled=True))
    return lax.psum_scatter(partial_terms, "tp", scatter_dimension=1, tiled=True)


def body(
    tokens,
    mix_gain,
    mix_value_w,
    mix_gate_w,
    mix_kernel,
    chan_gain,
    chan_bias,
    mix_out_w,
    ffn_gain,
    ffn_value_w,
    ffn_gate_w,
    ffn_value_kernel,
    ffn_gate_kernel,
    ffn_down_w,
):
    normed = rms_rows(collect_rows(tokens), mix_gain)
    mix_value, mix_gate = project_in(normed, mix_value_w, mix_gate_w)
    glu_rows = mix_value * jax.nn.sigmoid(mix_gate)
    mixed = along_positions(glu_rows, mix_kernel, SEQ_LEN)
    chan_sum, chan_square = lax.psum(
        (jnp.sum(mixed, axis=-1), jnp.sum(mixed * mixed, axis=-1)), "tp"
    )
    chan_mean = (chan_sum / CONV_W)[:, None]
    chan_var = jnp.maximum((chan_square / CONV_W)[:, None] - chan_mean * chan_mean, 0.0)
    active = jax.nn.silu(
        (mixed - chan_mean) * lax.rsqrt(chan_var + EPS) * chan_gain + chan_bias
    ).astype(jnp.bfloat16)
    middle = (tokens.astype(jnp.float32) + project_out(active, mix_out_w)).astype(jnp.bfloat16)
    normed_ffn = rms_rows(collect_rows(middle), ffn_gain)
    up_value, up_gate = project_in(normed_ffn, ffn_value_w, ffn_gate_w)
    up_value = along_positions(up_value, ffn_value_kernel, SEQ_LEN)
    up_gate = along_positions(up_gate, ffn_gate_kernel, SEQ_LEN)
    hidden = (jax.nn.silu(up_gate) * up_value).astype(jnp.bfloat16)
    return (middle.astype(jnp.float32) + project_out(hidden, ffn_down_w)).astype(jnp.bfloat16)


MESH = pl.DeviceIdType.MESH
UNIT_US = 0.36
HOP_US = 2.2


def chunk_plan(mix_cols, ffn_cols):
    wide = (2 * ffn_cols // 5) // 128 * 128
    rest = ffn_cols - 2 * wide
    plan = [
        ("mv", "A", mix_cols), ("mg", "A", mix_cols), ("mo", "B", mix_cols),
        ("vg0", "A", 2 * wide), ("vg1", "A", 2 * wide), ("vg2", "A", 2 * rest),
        ("w0", "A", wide), ("w1", "A", wide), ("w2", "B", rest),
    ]
    gates = {
        "vg0": ("mo", "u", 2), "vg1": ("vg0", "u", 1), "vg2": ("mg", "u", 2), "w0": ("mo", "u", 1),
        "w1": ("vg0", "u", 1), "w2": ("vg0", "u", 2),
    }
    return plan, gates, (wide, wide, rest)


def build_transfers(plan, gates, line):
    out = {}
    steps = range(1, line)
    for name, kind, cols in plan:
        out[(name, "1")] = dict(link="x", size=cols // 128, deps=[], phase="p1")
    for name, kind, cols in plan:
        width = cols // 128
        gate = [gates[name]] if name in gates else []
        late = [("mg", d, line - 1) for d in "ud"] if name in gates else []
        if kind == "A":
            for t in steps:
                for d in "ud":
                    deps = [(name, d, t - 1)] if t > 1 else [(name, "1")] + gate
                    out[(name, d, t)] = dict(link="z" + d, size=2 * width, deps=deps, phase="z")
            out[(name, "y", "o", 0)] = dict(link="y", size=2 * width, deps=[(name, "1")] + late, phase="y")
            for t in steps:
                for d in "ud":
                    out[(name, "y", d, t)] = dict(link="y", size=2 * width, deps=[(name, d, t)], phase="y")
        else:
            out[(name, "y", "o", 0)] = dict(link="y", size=2 * width, deps=[(name, "1")] + late, phase="y")
            for t in steps:
                for d in "ud":
                    deps = [(name, d, t - 1)] if t > 1 else [(name, "y", "o", 0)] + gate
                    out[(name, d, t)] = dict(link="z" + d, size=4 * width, deps=deps, phase="q")
    return out


def order_events(transfers, computes):
    free, arrival, seen, done = {}, {}, set(), {}
    program, now = [], 0.0

    def issue():
        for key, item in transfers.items():
            if key not in arrival and all(dep in seen for dep in item["deps"]):
                start = max(now, free.get(item["link"], 0.0))
                share = 0.5 if key[1] == "y" and key[2] != "o" else 1.0
                free[item["link"]] = start + share * item["size"] * UNIT_US
                arrival[key] = free[item["link"]] + HOP_US
                program.append(("send", key))
                if key == ("mo", "1"):
                    program.append(("compute", "tok_start"))
                    free["x"] += 5.6

    issue()
    program.append(("local", None))
    while len(seen) < len(transfers) or len(done) < len(computes):
        events = [(arrival[key], i, key) for i, key in enumerate(transfers) if key in arrival and key not in seen]
        ready = []
        for i, (name, needs, after, cost, delay) in enumerate(computes):
            if name in done or not all(a in done for a in after):
                continue
            if all(key in seen for key in transfers if key[0] in needs):
                ready.append((max([delay] + [done[a] + delay for a in after]), i, name, cost))
        can = [r for r in ready if r[0] <= now]
        if events and min(events)[0] <= now:
            pick = min(events)
        elif can:
            pick = min(can, key=lambda r: r[1])
        else:
            pick = min(events + ready, key=lambda r: r[0])
            now = max(now, pick[0])
        if len(pick) == 3:
            seen.add(pick[2])
            program.append(("recv", pick[2]))
            issue()
        else:
            program.append(("compute", pick[2]))
            now += pick[3]
            done[pick[2]] = now
    return program


def compute_list():
    items = [
        ("norm1_near", (), (), 1.2, 4.0),
        ("tok_fwd", (), (), 0.2, 9.5),
        ("norm1_far", (), ("tok_fwd",), 1.2, 1.2),
        ("mixv", ("mv",), ("norm1_near", "norm1_far"), 0.7, 0.0),
        ("mixg", ("mg",), ("mixv",), 0.7, 0.0),
        ("conv_a", (), ("mixg",), 1.7, 0.0),
        ("conv_b", (), ("conv_a",), 1.7, 0.0),
        ("stats", (), ("conv_b",), 0.4, 0.0),
        ("active_far", (), ("stats",), 0.6, 3.0),
        ("out_far", ("mo",), ("active_far",), 0.6, 0.0),
        ("active_near", (), ("out_far",), 0.6, 0.0),
        ("out_near", (), ("active_near",), 1.0, 0.0),
        ("out_x", (), ("out_near",), 0.4, 0.8),
        ("middle_a", (), ("out_x",), 0.4, 5.6),
        ("middle", (), ("middle_a",), 0.4, 5.4),
        ("norm2_near", (), ("middle",), 1.2, 1.2),
        ("mid_fwd", (), ("middle",), 0.2, 5.5),
        ("norm2_far", (), ("mid_fwd",), 1.2, 1.2),
    ]
    for side in ("far", "near"):
        for g in (0, 1, 2):
            items.append(("up_%s%d" % (side, g), ("vg%d" % g,), ("norm2_" + side,), (0.8, 0.8, 0.5)[g], 0.0))
        for g in (0, 1, 2):
            items.append(("down_%s%d" % (side, g), ("w%d" % g,), ("up_%s%d" % (side, g),), 0.4, 0.0))
        items.append(("send_" + side, (), tuple("down_%s%d" % (side, g) for g in (0, 1, 2)), 0.1, 0.0))
    items.append(("down_x", (), ("send_far",), 0.5, 1.0))
    items.append(("finish", (), ("down_x", "send_near"), 1.0, 7.5))
    return items


def layer_kernel(sizes, plan, groups, transfers, program, *refs):
    line, tok_rows, tok_cols, mix_cols, ffn_cols, taps, ffn_taps, total_cols = sizes
    (tokens, gain1, kern, cgain, cbias, gain2, vkern, gkern, packed) = refs[:9]
    out = refs[9]
    scratch = refs[10:]
    held = {item[0]: scratch[i] for i, item in enumerate(plan)}
    (tokall, midall, normed, mvbuf, pad, mixed, stat, stats_in, active,
     far_peer, far_mine, far_in, near_peer, near_mine, near_in, x_out, x_in,
     hid0, hid1, hid2, down_far_peer, down_far_mine, down_far_in,
     down_near_peer, down_near_mine, down_near_in, down_x_out, down_x_in,
     send_sem, recv_sem, loc_sem, act_send, act_recv) = scratch[len(plan):]
    hidden = (hid0, hid1, hid2)
    width = 2 * tok_cols
    offsets, at = {}, 0
    for name, _, cols in plan:
        offsets[name] = at
        at += cols
    cols_of = {item[0]: item[2] for item in plan}
    numbers = {key: i for i, key in enumerate(transfers)}
    fs = lax.axis_index("fs")
    core = lax.axis_index("tp")
    peer = 1 - core
    z, y, x = lax.div(fs, 4), lax.rem(lax.div(fs, 2), 2), lax.rem(fs, 2)
    far = 1 - x
    at_y, at_x = fs + 2 - 4 * y, fs + 1 - 2 * x
    half = line // 2

    barrier = pltpu.get_barrier_semaphore()
    for dev in ({"fs": at_y}, {"fs": at_x}, {"tp": peer}, {"fs": at_x, "tp": peer}):
        pl.semaphore_signal(barrier, inc=1, device_id=dev, device_id_type=MESH)

    @pl.when(z > 0)
    def _():
        pl.semaphore_signal(barrier, inc=1, device_id={"fs": fs - 4}, device_id_type=MESH)

    @pl.when(z < line - 1)
    def _():
        pl.semaphore_signal(barrier, inc=1, device_id={"fs": fs + 4}, device_id_type=MESH)

    def piece(name, part):
        lanes = pl.ds(pl.multiple_of(part * total_cols + offsets[name], 128), cols_of[name])
        return packed.at[:, lanes]

    local = []
    for i, (name, _, cols) in enumerate(plan):
        local.append(pltpu.make_async_copy(piece(name, x), held[name].at[z, y, x], loc_sem.at[i]))
    local.append(pltpu.make_async_copy(tokens, tokall.at[x, core], loc_sem.at[len(plan)]))
    for copy in local:
        copy.start()
    pl.semaphore_wait(barrier, 4 + jnp.minimum(z, 1) + jnp.minimum(line - 1 - z, 1))

    def guards(key, sending):
        phase = transfers[key]["phase"]
        if phase in ("z", "q"):
            d, t = key[1], key[2]
            if d == "u":
                return jnp.logical_and(z >= t - 1, z < line - 1) if sending else z >= t
            return jnp.logical_and(z <= line - t, z > 0) if sending else z <= line - 1 - t
        if phase == "y" and key[2] != "o":
            d, t = key[2], key[3]
            return z >= t if d == "u" else z <= line - 1 - t
        return None

    def make(key, sending):
        phase, name, i = transfers[key]["phase"], key[0], numbers[key]
        buf = held[name]
        src = None
        if phase in ("z", "q"):
            d, t = key[1], key[2]
            back = t - 1 if sending else t
            block = z - back if d == "u" else z + back
            dev = {"fs": fs + 4 if d == "u" else fs - 4}
            dst = buf.at[block, y] if phase == "z" else buf.at[block]
        elif phase == "y":
            d, t = key[2], key[3]
            block = z + t if d == "d" else z - t
            dev = {"fs": at_y}
            dst = buf.at[block, y if sending else 1 - y]
        else:
            dev = {"fs": at_x}
            dst = buf.at[z, y, x if sending else far]
            if sending:
                src = piece(name, far)
        return pltpu.make_async_remote_copy(
            src_ref=dst if src is None else src, dst_ref=dst, send_sem=send_sem.at[i],
            recv_sem=recv_sem.at[i], device_id=dev, device_id_type=MESH,
        )

    def act(key, sending, what):
        guard = guards(key, sending)

        def run():
            what(make(key, sending))

        if guard is None:
            run()
        else:
            pl.when(guard)(run)

    acts = []

    def exchange(src, dst, landed, **dev):
        i = len(acts)
        acts.append(None)

        def build(s, d):
            return pltpu.make_async_remote_copy(
                src_ref=s, dst_ref=d, send_sem=act_send.at[i], recv_sem=act_recv.at[i],
                device_id=dev, device_id_type=MESH,
            )

        acts[i] = build(src, dst)
        return build(src, dst).start, build(landed, landed).wait_recv

    tok_core = exchange(tokens, tokall.at[x, core], tokall.at[x, peer], tp=peer)
    tok_x = exchange(tokens, tokall.at[x, core], tokall.at[far, core], fs=at_x)
    tok_fwd = exchange(tokall.at[far, core], tokall.at[far, core], tokall.at[far, peer], tp=peer)
    mid_core = exchange(midall.at[x, core], midall.at[x, core], midall.at[x, peer], tp=peer)
    mid_x = [
        exchange(midall.at[x, core, r], midall.at[x, core, r], midall.at[far, core, r], fs=at_x)
        for r in (pl.ds(0, tok_rows // 2), pl.ds(tok_rows // 2, tok_rows // 2))
    ]
    mid_fwd = exchange(midall.at[far, core], midall.at[far, core], midall.at[far, peer], tp=peer)
    stat_all = [
        exchange(stat, stats_in.at[0], stats_in.at[0], tp=peer),
        exchange(stat, stats_in.at[1], stats_in.at[1], fs=at_x),
        exchange(stat, stats_in.at[2], stats_in.at[2], fs=at_x, tp=peer),
    ]
    out_far = exchange(far_peer, far_in, far_in, tp=peer)
    out_near = exchange(near_peer, near_in, near_in, tp=peer)
    cut = tok_rows // 2
    top, low = pl.ds(0, cut), pl.ds(cut, cut)
    out_x = [exchange(x_out.at[r], x_in.at[r], x_in.at[r], fs=at_x) for r in (top, low)]
    down_far = exchange(down_far_peer, down_far_in, down_far_in, tp=peer)
    down_near = exchange(down_near_peer, down_near_in, down_near_in, tp=peer)
    down_x = exchange(down_x_out, down_x_in, down_x_in, fs=at_x)

    def norm_rows(rows_of, gain, side):
        def block(r, carry):
            at_rows = pl.ds(pl.multiple_of(r * 64, 64), 64)
            a = rows_of[side, 0, at_rows, :].astype(jnp.float32)
            b = rows_of[side, 1, at_rows, :].astype(jnp.float32)
            total = jnp.sum(a * a + b * b, axis=-1, keepdims=True)
            scale = lax.rsqrt(total / width + EPS)
            normed[0, side, at_rows, :] = (a * scale * gain[0]).astype(jnp.bfloat16)
            normed[1, side, at_rows, :] = (b * scale * gain[1]).astype(jnp.bfloat16)
            return carry

        lax.fori_loop(0, tok_rows // 64, block, 0)

    def project(name, lo, hi, side=None):
        total = None
        for h in (0, 1):
            weight = held[name][h * half:(h + 1) * half, :, :, :, lo:hi]
            weight = weight.reshape(-1, hi - lo)
            left = normed[h].reshape(2 * tok_rows, tok_cols) if side is None else normed[h, side]
            term = jnp.dot(left, weight, preferred_element_type=jnp.float32)
            total = term if total is None else total + term
        return total

    def project_back(left, name, side):
        weight = held[name][pl.ds(side * half, half)]
        weight = weight.reshape(-1, weight.shape[-1])
        return lax.dot_general(left, weight, (((1,), (1,)), ((), ())), preferred_element_type=jnp.float32)

    def start_tokens():
        tok_core[0]()
        tok_x[0]()

    def forward_tokens():
        tok_x[1]()
        tok_fwd[0]()

    def norm1_near():
        pad[...] = jnp.zeros_like(pad)
        tok_core[1]()
        norm_rows(tokall, gain1, x)

    def norm1_far():
        tok_fwd[1]()
        norm_rows(tokall, gain1, far)

    seqs = 2 * tok_rows // SEQ_LEN
    lead = -(-(taps // 2) // 8) * 8

    def mixv():
        mvbuf[...] = project("mv", 0, mix_cols)

    def mixg():
        glu = mvbuf[...] * jax.nn.sigmoid(project("mg", 0, mix_cols))
        pad[:, lead:lead + SEQ_LEN, :] = glu.reshape(seqs, SEQ_LEN, mix_cols)

    lane_blocks = mix_cols // 128

    def conv(lo, hi):
        def block(i, carry):
            s, c = lo + lax.div(i, lane_blocks), lax.rem(i, lane_blocks)
            lanes = pl.ds(pl.multiple_of(c * 128, 128), 128)
            taps_at = pl.ds(pl.multiple_of(x * mix_cols + c * 128, 128), 128)
            total = jnp.zeros((SEQ_LEN, 128), jnp.float32)
            for k in range(taps):
                total = total + pad[s, pl.ds(lead - taps // 2 + k, SEQ_LEN), lanes] * kern[k:k + 1, taps_at]
            mixed[pl.ds(pl.multiple_of(s * SEQ_LEN, SEQ_LEN), SEQ_LEN), lanes] = total
            return carry

        lax.fori_loop(0, (hi - lo) * lane_blocks, block, 0)

    def stats():
        for r in range(0, 2 * tok_rows, 128):
            v = mixed[r:r + 128, :]
            first = jnp.sum(v, axis=-1, keepdims=True)
            second = jnp.sum(v * v, axis=-1, keepdims=True)
            lane = lax.broadcasted_iota(jnp.int32, (128, 128), 1)
            stat[:, r:r + 128] = jnp.where(lane == 0, first, second).T[:8]
        for send, _ in stat_all:
            send()

    def make_active(side, first):
        if first:
            for _, wait in stat_all:
                wait()
        for r in range(0, tok_rows, 128):
            at_rows = pl.ds(pl.multiple_of(side * tok_rows + r, 128), 128)
            both = stat[:, at_rows] + stats_in[0, :, at_rows] + (stats_in[1, :, at_rows] + stats_in[2, :, at_rows])
            both = jnp.concatenate([both] * 16, axis=0).T
            mean = both[:, 0:1] / (4 * mix_cols)
            var = jnp.maximum(both[:, 1:2] / (4 * mix_cols) - mean * mean, 0.0)
            v = (mixed[at_rows, :] - mean) * lax.rsqrt(var + EPS) * cgain[x] + cbias[x]
            active[at_rows, :] = (v * jax.nn.sigmoid(v)).astype(jnp.bfloat16)

    def rows_at(side):
        return pl.ds(pl.multiple_of(side * tok_rows, tok_rows), tok_rows)

    def make_out_far():
        left = active[rows_at(far), :]
        far_peer[...] = project_back(left, "mo", peer)
        out_far[0]()
        far_mine[...] = project_back(left, "mo", core)

    def make_out_near():
        out_far[1]()
        x_out[...] = far_mine[...] + far_in[...]
        out_x[0][0]()
        out_x[1][0]()
        left = active[rows_at(x), :]
        near_peer[...] = project_back(left, "mo", peer)
        out_near[0]()
        near_mine[...] = project_back(left, "mo", core)

    def make_out_x():
        out_near[1]()
        near_mine[...] += near_in[...]

    def make_middle(part, rows):
        out_x[part][1]()
        total = tokens[rows, :].astype(jnp.float32) + (near_mine[rows, :] + x_in[rows, :])
        midall[x, core, rows, :] = total.astype(jnp.bfloat16)
        mid_x[part][0]()
        if part:
            mid_core[0]()

    def forward_middle():
        mid_x[0][1]()
        mid_x[1][1]()
        mid_fwd[0]()

    def norm2_near():
        mid_core[1]()
        norm_rows(midall, gain2, x)

    def norm2_far():
        mid_fwd[1]()
        norm_rows(midall, gain2, far)

    def short_conv(values, kernel_rows, lanes):
        pos = lax.rem(lax.broadcasted_iota(jnp.int32, values.shape, 0), SEQ_LEN)
        total = None
        for k in range(ffn_taps):
            shift = k - ffn_taps // 2
            term = values
            if shift:
                term = pltpu.roll(values, (-shift) % tok_rows, 0)
                inside = pos < SEQ_LEN - shift if shift > 0 else pos >= -shift
                term = jnp.where(inside, term, 0.0)
            term = term * kernel_rows[k:k + 1, lanes]
            total = term if total is None else total + term
        return total

    def up(g, side):
        count = groups[g]
        start = sum(groups[:g])
        for c in range(0, count, 256):
            n = min(256, count - c)
            lanes = pl.ds(pl.multiple_of(x * ffn_cols + start + c, 128), n)
            name = "vg%d" % g
            value = short_conv(project(name, c, c + n, side), vkern, lanes)
            gate = short_conv(project(name, count + c, count + c + n, side), gkern, lanes)
            hidden[g][side, :, c:c + n] = (gate * jax.nn.sigmoid(gate) * value).astype(jnp.bfloat16)

    fresh = set()

    def down(g, where, name, peer_buf, mine_buf):
        left = hidden[g][where]
        for side, buf in ((peer, peer_buf), (core, mine_buf)):
            term = project_back(left, "w%d" % g, side)
            if name in fresh:
                buf[...] += term
            else:
                buf[...] = term
        fresh.add(name)

    def make_down_x():
        down_far[1]()
        down_x_out[...] = (down_far_mine[...] + down_far_in[...]).astype(jnp.bfloat16)
        down_x[0]()

    def finish():
        down_near[1]()
        near = down_near_mine[...] + down_near_in[...] + midall[x, core].astype(jnp.float32)
        down_near_mine[...] = near
        down_x[1]()
        out[...] = (down_near_mine[...] + down_x_in[...].astype(jnp.float32)).astype(jnp.bfloat16)

    run = {
        "tok_start": start_tokens, "tok_fwd": forward_tokens, "norm1_near": norm1_near, "norm1_far": norm1_far,
        "mixv": mixv, "mixg": mixg, "conv_a": lambda: conv(0, seqs // 2), "conv_b": lambda: conv(seqs // 2, seqs),
        "stats": stats, "active_far": lambda: make_active(far, True), "active_near": lambda: make_active(x, False),
        "out_far": make_out_far, "out_near": make_out_near, "out_x": make_out_x, "middle_a": lambda: make_middle(0, top), "middle": lambda: make_middle(1, low),
        "mid_fwd": forward_middle, "norm2_near": norm2_near, "norm2_far": norm2_far,
        "send_far": down_far[0], "send_near": down_near[0], "down_x": make_down_x, "finish": finish,
    }
    for g in (0, 1, 2):
        run["up_far%d" % g] = functools.partial(up, g, far)
        run["up_near%d" % g] = functools.partial(up, g, x)
        run["down_far%d" % g] = functools.partial(down, g, far, "far", down_far_peer, down_far_mine)
        run["down_near%d" % g] = functools.partial(down, g, x, "near", down_near_peer, down_near_mine)

    for kind, key in program:
        if kind == "send":
            act(key, True, lambda copy: copy.start())
        elif kind == "recv":
            act(key, False, lambda copy: copy.wait_recv())
        elif kind == "local":
            for copy in local:
                copy.wait()
        else:
            run[key]()
    for key in transfers:
        act(key, True, lambda copy: copy.wait_send())
    for copy in acts:
        copy.wait_send()


def fused_body(fs_size, tokens, mix_gain, mix_value_w, mix_gate_w, mix_kernel, chan_gain, chan_bias, mix_out_w,
               ffn_gain, ffn_value_w, ffn_gate_w, ffn_value_kernel, ffn_gate_kernel, ffn_down_w):
    rows, mix_cols = mix_value_w.shape[0], mix_value_w.shape[1] // 2
    ffn_cols = ffn_value_w.shape[1] // 2
    tok_rows, tok_cols = tokens.shape
    line = fs_size // 4
    plan, gates, groups = chunk_plan(mix_cols, ffn_cols)
    transfers = build_transfers(plan, gates, line)
    program = order_events(transfers, compute_list())
    bf16, f32 = jnp.bfloat16, jnp.float32
    parts = []
    for q in (0, 1):
        for weight in (mix_value_w, mix_gate_w, mix_out_w.T):
            parts.append(weight[:, q * mix_cols:(q + 1) * mix_cols])
        cuts = [q * ffn_cols + sum(groups[:g]) for g in (0, 1, 2)]
        for g in (0, 1, 2):
            for weight in (ffn_value_w, ffn_gate_w):
                parts.append(weight[:, cuts[g]:cuts[g] + groups[g]])
        parts.append(ffn_down_w.T[:, q * ffn_cols:(q + 1) * ffn_cols])
    packed = jnp.concatenate([part.astype(bf16) for part in parts], axis=1)
    sizes = (line, tok_rows, tok_cols, mix_cols, ffn_cols, mix_kernel.shape[0], ffn_value_kernel.shape[0],
             packed.shape[1] // 2)
    vm = pltpu.VMEM
    lead = -(-(mix_kernel.shape[0] // 2) // 8) * 8
    both = 2 * tok_rows
    full = (tok_rows, tok_cols)
    sums = [vm(full, f32)] * 6
    scratch = [vm((line, 2, 2, rows, item[2]), bf16) for item in plan] + [
        vm((2, 2) + full, bf16), vm((2, 2) + full, bf16), vm((2, 2) + full, bf16),
        vm((both, mix_cols), f32), vm((both // SEQ_LEN, SEQ_LEN + 2 * lead, mix_cols), f32),
        vm((both, mix_cols), f32), vm((8, both), f32), vm((3, 8, both), f32), vm((both, mix_cols), bf16),
    ] + sums + [vm(full, f32)] * 2 + [vm((2, tok_rows, g), bf16) for g in groups] + sums + [vm(full, bf16)] * 2 + [
        pltpu.SemaphoreType.DMA((len(transfers),)), pltpu.SemaphoreType.DMA((len(transfers),)),
        pltpu.SemaphoreType.DMA((len(plan) + 1,)), pltpu.SemaphoreType.DMA((17,)), pltpu.SemaphoreType.DMA((17,)),
    ]
    return pl.pallas_call(
        functools.partial(layer_kernel, sizes, plan, groups, transfers, program),
        out_shape=jax.ShapeDtypeStruct(full, bf16),
        in_specs=[pl.BlockSpec(memory_space=vm)] * 9,
        out_specs=pl.BlockSpec(memory_space=vm),
        scratch_shapes=scratch,
        compiler_params=pltpu.CompilerParams(
            collective_id=0, has_side_effects=True, vmem_limit_bytes=56 * 1024 * 1024
        ),
    )(
        tokens, mix_gain.reshape(2, 1, tok_cols), mix_kernel, chan_gain.reshape(2, 1, -1),
        chan_bias.reshape(2, 1, -1), ffn_gain.reshape(2, 1, tok_cols), ffn_value_kernel, ffn_gate_kernel, packed,
    )


def pick_body(fs_size, tp_size):
    def run(*args):
        tokens, mix_w, ffn_w = args[0], args[2], args[9]
        fits = (
            tp_size == 2 and fs_size % 8 == 0 and fs_size <= 32
            and mix_w.shape[0] % 16 == 0 and mix_w.shape[1] % 256 == 0
            and ffn_w.shape[1] % 256 == 0 and ffn_w.shape[1] >= 1024
            and tokens.shape[0] % 64 == 0 and tokens.shape[1] % 128 == 0
            and fs_size * mix_w.shape[0] == tp_size * tokens.shape[1]
            and fs_size * args[7].shape[1] == tp_size * tokens.shape[1]
        )
        if fits:
            return fused_body(fs_size, *args)
        return body(*args)

    return run


def solution(mesh):
    return jax.shard_map(
        pick_body(mesh.shape["fs"], mesh.shape["tp"]),
        mesh=mesh,
        in_specs=(
            P("fs", "tp"),
            P(),
            P("fs", "tp"),
            P("fs", "tp"),
            P(None, "tp"),
            P("tp"),
            P("tp"),
            P("tp", "fs"),
            P(),
            P("fs", "tp"),
            P("fs", "tp"),
            P(None, "tp"),
            P(None, "tp"),
            P("tp", "fs"),
        ),
        out_specs=P("fs", "tp"),
        check_vma=False,
    )
```
